512 devices in a mesh: sp: 64 (over z, y), tp: 8 (over x, core).
Axes of the slice: x: 4, y: 8, z: 8, core: 2. Of those that a mesh axis runs over, the one named last changes fastest.
Arguments:
- block_input: bfloat16 [32768, 2048], P('sp'), may hold values from -6 to 6
- value_weight: bfloat16 [2048, 2048], P(None, 'tp'), may hold values from -0.125 to 0.125
- queries: bfloat16 [32768, 1024], P('sp', 'tp'), may hold values from -0.5 to 0.5
- key_rows: bfloat16 [32768, 1024], P('sp', 'tp'), may hold values from -0.5 to 0.5
- log_decay: float32 [32768, 32], P('sp', 'tp'), may hold values from -0.125 to 0, as said below
- out_grad: bfloat16 [32768, 2048], P('sp', 'tp'), may hold values from -6 to 6
Outputs:
- query_grad: float32 [32768, 1024], P('sp', 'tp')
- key_grad: float32 [32768, 1024], P('sp', 'tp')
- decay_grad: float32 [32768, 32], P('sp', 'tp')
- weight_grad: float32 [2048, 2048], P('sp', 'tp')
- row_norms: float32 [2048], P('sp')
The draws below stay inside these ranges and needn't reach their ends.
Inputs may be any that keep to these rules, and one draw needn't show every extreme that they name: `log_decay`: log decays of each position and head, never positive.
All inputs are finite; a program needn't handle non-finite values.
Results may differ from the reference program's by a relative error of at most 0.013.
Values sent between devices are 32-bit elements; how exact they have to be, the bound alone decides.
A program may use at most 64 MiB of HBM per device.

```python
import jax
import jax.numpy as jnp
from jax import lax

D = 2048
HEADS = 32
GROUPS = 8
HEAD_DIM = 64
STATE = 128
SPAN = 128
TOKENS = 32768


def draw_log_decay(key, part):
    pick_key, slow_key, fast_key, block_key, rough_key = jax.random.split(key, 5)
    fast_share = 0.5
    quick = jax.random.uniform(pick_key, (HEADS,)) < fast_share
    slow_rate = jax.random.uniform(slow_key, (HEADS,), minval=0.5, maxval=1.5) / TOKENS
    fast_rate = jax.random.uniform(fast_key, (HEADS,), minval=0.01, maxval=0.04)
    base_rate = jnp.where(quick, fast_rate, slow_rate)
    block_scale = jnp.exp(jax.random.uniform(block_key, (TOKENS // SPAN, HEADS), minval=-0.69, maxval=0.69))
    block_scale = jnp.repeat(block_scale, SPAN, axis=0)
    roughness = jax.random.uniform(rough_key, (TOKENS, HEADS), minval=0.5, maxval=1.5)
    return (-(base_rate[None, :] * block_scale * roughness)).astype(jnp.float32)


def levels(stream_key, dims, shards, low, largest):
    def one(position, parts):
        heights = jax.random.uniform(jax.random.fold_in(jax.random.fold_in(stream_key, 6), position), (parts,), jnp.float32, low / len(shards), largest / len(shards))
        return jnp.repeat(jnp.exp(heights), dims[position] // parts).reshape((-1,) + (1,) * (len(dims) - position - 1))

    loudness = one(*shards[0])
    for cut in shards[1:]:
        loudness = loudness * one(*cut)
    return loudness


def noise(own_key, shape, scale, limit, cuts=(), kind=jnp.bfloat16):
    level = levels(own_key, shape, cuts, -0.22, 0.18) if cuts else 1.0
    drawn = jax.random.normal(own_key, shape, jnp.float32) * scale * level
    return jnp.minimum(jnp.maximum(drawn, -limit), limit).astype(kind)


def setup_inputs(seed: int = 0) -> dict:
    arg_keys = jax.random.split(jax.random.key(seed), 7)
    block_input = noise(arg_keys[0], (TOKENS, D), 1.0, 6.0, ((0, 64),))
    value_weight = noise(arg_keys[1], (D, HEADS * HEAD_DIM), D ** -0.5, 0.125, ((1, 8),))
    queries = noise(arg_keys[2], (TOKENS, GROUPS * STATE), STATE ** -0.5, 0.5, ((0, 64), (1, 8)))
    key_rows = noise(arg_keys[3], (TOKENS, GROUPS * STATE), STATE ** -0.5, 0.5, ((0, 64), (1, 8)))
    log_decay = draw_log_decay(jax.random.fold_in(arg_keys[6], 71), 0)
    out_grad = noise(arg_keys[5], (TOKENS, HEADS * HEAD_DIM), 1.0, 6.0, ((0, 64), (1, 8)))
    return {"block_input": block_input, "value_weight": value_weight, "queries": queries, "key_rows": key_rows, "log_decay": log_decay, "out_grad": out_grad}


exact_mode = lax.Precision.HIGHEST

def block_step(memory, pieces):
    queries, key_rows, decays, values = pieces
    length = decays.shape[0]
    cumulative = jnp.cumsum(decays, axis=0)
    causal = (lax.iota(jnp.int32, length)[:, None] >= lax.iota(jnp.int32, length)[None, :])[:, :, None, None]
    log_gap = cumulative[:, None] - cumulative[None, :]
    weights = jnp.where(causal, jnp.exp(jnp.where(causal, log_gap, 0.0)), 0.0)
    scores = jnp.einsum('sgn,rgn->srg', queries, key_rows, precision=exact_mode)
    within = jnp.einsum('srgj,rgjp->sgjp', scores[..., None] * weights, values, precision=exact_mode)
    carried = jnp.einsum('sgn,gjpn->sgjp', queries, memory, precision=exact_mode) * jnp.exp(cumulative)[..., None]
    to_end = jnp.exp(cumulative[-1] - cumulative)
    fresh_state = jnp.einsum('rgn,rgjp->gjpn', key_rows, values * to_end[..., None], precision=exact_mode)
    new_memory = jnp.exp(cumulative[-1])[..., None, None] * memory + fresh_state
    return (new_memory, within + carried)

def reference(block_input, value_weight, queries, key_rows, log_decay, out_grad):
    values = jnp.dot(block_input, value_weight, preferred_element_type=jnp.float32).astype(jnp.bfloat16)
    total = queries.shape[0]
    groups = queries.shape[1] // STATE
    heads = log_decay.shape[1]
    per_group = heads // groups
    blocks = total // SPAN
    memory = jnp.zeros((groups, per_group, HEAD_DIM, STATE), jnp.float32)

    def forward(query_in, key_in, decay_in, value_in):
        pieces = (query_in.reshape(blocks, SPAN, groups, STATE), key_in.reshape(blocks, SPAN, groups, STATE), decay_in.reshape(blocks, SPAN, groups, per_group), value_in.reshape(blocks, SPAN, groups, per_group, HEAD_DIM))
        final, outputs = lax.scan(block_step, memory, pieces)
        return outputs.reshape(total, heads * HEAD_DIM)
    mixed, pullback = jax.vjp(forward, queries.astype(jnp.float32), key_rows.astype(jnp.float32), log_decay, values.astype(jnp.float32))
    query_grad, key_grad, decay_grad, value_grad = pullback(out_grad.astype(jnp.float32))
    rounded_grad = value_grad.astype(jnp.bfloat16)
    weight_grad = jnp.dot(block_input.T, rounded_grad, preferred_element_type=jnp.float32)
    row_norms = lax.optimization_barrier(jnp.sum(weight_grad * weight_grad, axis=1))
    return (query_grad, key_grad, decay_grad, weight_grad, row_norms)
```

```python
import functools

import jax
import jax.numpy as jnp
from jax import lax
from jax.experimental import pallas as pl
from jax.experimental.pallas import tpu as pltpu
from jax.sharding import Mesh
from jax.sharding import PartitionSpec as P

SP = ("sp_0", "sp_1")
F32 = jnp.float32
BF16 = jnp.bfloat16
MESH = pl.DeviceIdType.MESH
LOADS = 4
CHUNKS = 4
ORDER = (2, 1, 3, 0)


def dot(a, b, a_dim, b_dim):
    return lax.dot_general(a, b, (((a_dim,), (b_dim,)), ((), ())), preferred_element_type=F32)


def thirds(x):
    high = x.astype(BF16)
    rest = x - high.astype(F32)
    middle = rest.astype(BF16)
    low = (rest - middle.astype(F32)).astype(BF16)
    return high, middle, low


def far_first(n):
    return sorted(range(n), key=lambda d: -min(d, n - d))


def kernel(
    nz, ny, nt,
    decay_hbm, grad_hbm, query_hbm, key_hbm, input_hbm, weight_hbm,
    query_grad, key_grad, decay_grad, weight_grad, norms,
    decay, grad, query, key, block_in, weight,
    value, value_of, grad_of, rise, fall, grad_rise, value_fall, tri, down, across,
    send_b, recv_b, out_b, in_b, send_f, recv_f, out_f, in_f,
    own_state, state_grad, values_grad, mixed, local_q, local_k, rounded,
    turned_a, turned_b, partial_a, partial_b, ring_ap, ring_am, ring_bp, ring_bm,
    block_a, block_b, last_a, last_b, norm_out, norm_in,
    load_sem, scan_send, scan_recv, ring_send, ring_recv, last_send, last_recv, norm_send, norm_recv,
):
    z, y, t = lax.axis_index("sp_0"), lax.axis_index("sp_1"), lax.axis_index("tp")
    shards = nz * ny
    me = z * ny + y
    rows, width = grad.shape
    heads = decay.shape[0]
    depth = width // heads
    pair = 2 * depth
    state = query.shape[1]
    piece = rows // LOADS

    loads = [
        pltpu.make_async_copy(decay_hbm, decay, load_sem.at[0]),
        pltpu.make_async_copy(grad_hbm, grad, load_sem.at[1]),
        pltpu.make_async_copy(query_hbm, query, load_sem.at[2]),
        pltpu.make_async_copy(weight_hbm, weight, load_sem.at[3]),
        pltpu.make_async_copy(key_hbm, key, load_sem.at[4]),
    ]
    for i in range(LOADS):
        part = pl.ds(i * piece, piece)
        loads.append(pltpu.make_async_copy(input_hbm.at[part], block_in.at[part], load_sem.at[5 + i]))
    for copy in loads:
        copy.start()

    barrier = pltpu.get_barrier_semaphore()

    def greet(i, carry):
        other = lax.rem(me + i, shards)
        pl.semaphore_signal(
            barrier, inc=1, device_id={"sp_0": lax.div(other, ny), "sp_1": lax.rem(other, ny)}, device_id_type=MESH
        )
        return carry

    lax.fori_loop(1, shards, greet, 0)
    for j in range(1, nt):
        pl.semaphore_signal(barrier, inc=1, device_id={"tp": lax.rem(t + j, nt)}, device_id_type=MESH)

    def exchange(source, target, number):
        def one(dz, dy):
            oz, oy = lax.rem(z + dz, nz), lax.rem(y + dy, ny)
            pltpu.make_async_remote_copy(
                src_ref=source.at[oz * ny + oy], dst_ref=target.at[me],
                send_sem=scan_send.at[number], recv_sem=scan_recv.at[number],
                device_id={"sp_0": oz, "sp_1": oy}, device_id_type=MESH,
            ).start()

        def plane(i, carry):
            for dy in far_first(ny):
                one(1 + lax.rem(i + nz // 2 - 1, nz - 1), dy)
            return carry

        lax.fori_loop(0, nz - 1, plane, 0)
        for dy in far_first(ny):
            if dy:
                one(0, dy)
        target[me] = source[me]

    def arrived(buffer, sem):
        pltpu.make_async_copy(buffer, buffer, sem).wait()

    early = lax.broadcasted_iota(jnp.int32, (rows, rows), 0) <= lax.broadcasted_iota(jnp.int32, (rows, rows), 1)
    tri[...] = jnp.where(early, 1.0, 0.0).astype(BF16)

    def stacked(x):
        high, middle, low = thirds(x)
        return jnp.concatenate(
            [high.astype(F32), middle.astype(F32), low.astype(F32), jnp.zeros_like(x)], axis=0
        ).astype(BF16)

    def unstacked(x):
        return x[0:8] + x[8:16] + x[16:24]

    loads[0].wait()
    log8 = jnp.concatenate([decay[...]] * (8 // heads), axis=0)
    across[...] = unstacked(dot(stacked(log8), tri[...], 1, 0))
    down[...] = jnp.concatenate([across[...]] * 16, axis=0).T
    lane = lax.broadcasted_iota(jnp.int32, (rows, pair), 1)
    for h in range(0, heads, 2):
        cols = pl.ds(h * depth, pair)
        cum = jnp.where(
            lane < depth,
            jnp.broadcast_to(down[:, h : h + 1], (rows, pair)),
            jnp.broadcast_to(down[:, h + 1 : h + 2], (rows, pair)),
        )
        rise[:, cols] = jnp.exp(cum)
        fall[:, cols] = jnp.exp(cum[rows - 1 : rows, :] - cum)

    loads[1].wait()
    loads[2].wait()
    grad_rise[...] = (grad[...].astype(F32) * rise[...]).astype(BF16)
    own = dot(grad_rise[...], query[...], 0, 0)
    for h in range(heads):
        send_b[:, h, :] = own[h * depth : (h + 1) * depth, :]
    send_b[:, heads, :] = jnp.broadcast_to(down[rows - 1 : rows, :], (shards, state))
    pl.semaphore_wait(barrier, shards - 1 + nt - 1)
    exchange(send_b, recv_b, 0)

    loads[3].wait()
    for i in range(LOADS):
        loads[5 + i].wait()
        part = pl.ds(i * piece, piece)
        value[part, :] = dot(block_in[part, :], weight[...], 1, 0).astype(BF16)
    loads[4].wait()
    value_fall[...] = (value[...].astype(F32) * fall[...]).astype(BF16)
    own_state[...] = dot(value_fall[...], key[...], 0, 0)
    for h in range(heads):
        send_f[:, h, :] = own_state[h * depth : (h + 1) * depth, :]
    exchange(send_f, recv_f, 1)

    tall_a, tall_b = turned_a.shape[1], turned_b.shape[1]
    small = tall_a // ny
    for i in range(nz):
        turned_a[i] = block_in[:, i * tall_a : (i + 1) * tall_a].T
    for i in range(nz):
        for j in range(ny):
            turned_b[j, i * small : (i + 1) * small, :] = turned_a[i, j * small : (j + 1) * small, :]
    for h in range(heads):
        cols = pl.ds((h // 2) * pair, pair)
        mine = (lane < depth) if h % 2 == 0 else (lane >= depth)
        grad_of[h] = jnp.where(mine, grad[:, cols].astype(F32), 0.0).astype(BF16)
        value_of[h] = jnp.where(mine, value[:, cols].astype(F32), 0.0).astype(BF16)

    def first(buffer):
        return buffer.at[pl.ds(0, shards - 1)]

    arrived(first(recv_b), scan_recv.at[0])
    logs = recv_b[:, heads, :]
    logs = jnp.concatenate([logs] * (128 // shards), axis=0).T
    factors = jnp.exp(logs[0:heads, :])

    def factor(k):
        return jnp.broadcast_to(factors[:, k : k + 1], (heads, state))

    total = jnp.zeros((heads, state), F32)
    for k in reversed(range(shards)):
        out_b[k] = total
        if k:
            total = factor(k) * total + recv_b[k, 0:heads, :]
    exchange(out_b, in_b, 2)

    arrived(first(recv_f), scan_recv.at[1])
    total = jnp.zeros((heads, state), F32)
    for k in range(shards):
        out_f[k] = total
        if k < shards - 1:
            total = factor(k) * total + recv_f[k]
    exchange(out_f, in_f, 3)

    half = rows // 2
    causal = lax.broadcasted_iota(jnp.int32, (half, half), 0) >= lax.broadcasted_iota(jnp.int32, (half, half), 1)
    for late, early_block in ((0, 0), (1, 0), (1, 1)):
        to, of = pl.ds(late * half, half), pl.ds(early_block * half, half)
        scores = dot(query[to, :], key[of, :], 1, 1)
        score_grad = jnp.zeros((half, half), F32)
        for h0 in range(0, heads, 2):
            cols = pl.ds(h0 * depth, pair)
            for h in (h0, h0 + 1):
                gap = jnp.broadcast_to(down[to, h : h + 1], (half, half)) - jnp.broadcast_to(
                    across[h : h + 1, of], (half, half)
                )
                decayed = jnp.exp(jnp.minimum(gap, 0.0))
                if late == early_block:
                    decayed = jnp.where(causal, decayed, 0.0)
                score_grad += dot(grad_of[h, to, :], value[of, cols], 1, 1) * decayed
                weighted = (scores * decayed).astype(BF16)
                to_value = dot(weighted, grad_of[h, to, :], 0, 0)
                to_mixed = dot(weighted, value_of[h, of, :], 1, 0)
                if h == h0 and late == early_block:
                    if late == 0:
                        values_grad[of, cols] = to_value
                    else:
                        values_grad[of, cols] = to_value
                else:
                    values_grad[of, cols] += to_value
                if h == h0 and early_block == 0:
                    mixed[to, cols] = to_mixed
                else:
                    mixed[to, cols] += to_mixed
        score_grad = score_grad.astype(BF16)
        to_q = dot(score_grad, key[of, :], 1, 0)
        to_k = dot(score_grad, query[to, :], 0, 0)
        if early_block == 0:
            local_q[to, :] = to_q
        else:
            local_q[to, :] += to_q
        if late == early_block:
            local_k[of, :] = to_k
        else:
            local_k[of, :] += to_k

    arrived(first(in_b), scan_recv.at[2])
    for h in range(heads):
        state_grad[h * depth : (h + 1) * depth, :] = in_b[:, h, :]
    state_grad_16 = state_grad[...].astype(BF16)
    values_grad[...] += fall[...] * dot(key[...], state_grad_16, 1, 1)
    rounded[...] = values_grad[...].astype(BF16)

    axes = (
        ("sp_0", nz, z, "sp_1", ny, y, turned_a, partial_a, (ring_ap, ring_am), block_a, last_a),
        ("sp_1", ny, y, "sp_0", nz, z, turned_b, partial_b, (ring_bp, ring_bm), block_b, last_b),
    )
    reach = ring_ap.shape[0]

    def product(a, r):
        _, n, at, _, n_o, at_o, turned, partial, _, _, _ = axes[a]
        block = dot(turned[lax.rem(at + r, n)], rounded[:, a * pair : (a + 1) * pair], 1, 0)
        for q in range(n_o):
            where = pl.multiple_of(lax.rem(q + n_o - at_o, n_o) * small, small)
            partial[r, pl.ds(where, small), :] = block[q * small : (q + 1) * small, :]

    def comes(way, s, c):
        return s > 0 or (c < CHUNKS // 2) == (way == 0)

    def slot(a, way, s, c):
        return ((a * 2 + way) * reach + s) * CHUNKS + c

    def span(a, c):
        tall = axes[a][7].shape[1] // CHUNKS
        return pl.ds(c * tall, tall)

    def block_of(a, way, s):
        n = axes[a][1]
        return reach - s if way == 0 else n - reach + s

    def hop(a, way, s, c):
        name, n, at, _, _, _, _, partial, ring, _, _ = axes[a]
        pltpu.make_async_remote_copy(
            src_ref=partial.at[block_of(a, way, s), span(a, c)], dst_ref=ring[way].at[s, span(a, c)],
            send_sem=ring_send.at[a], recv_sem=ring_recv.at[slot(a, way, s, c)],
            device_id={name: lax.rem(at + (1 if way == 0 else n - 1), n)}, device_id_type=MESH,
        ).start()

    def landed(a, way, s, c):
        arrived(axes[a][8][way].at[s, span(a, c)], ring_recv.at[slot(a, way, s, c)])
        return axes[a][8][way][s, span(a, c), :]

    def finish_queries():
        arrived(first(in_f), scan_recv.at[3])
        before = jnp.concatenate([in_f[:, h, :] for h in range(heads)], axis=0)
        query_grad[...] = local_q[...] + dot(grad_rise[...], before.astype(BF16), 1, 0)

    def finish_keys():
        key_grad[...] = local_k[...] + dot(value_fall[...], state_grad[...].astype(BF16), 1, 0)

    def finish_decays():
        before = jnp.concatenate([in_f[:, h, :] for h in range(heads)], axis=0)
        whole = mixed[...] + rise[...] * dot(query[...], before.astype(BF16), 1, 1)
        change = grad[...].astype(F32) * whole - value[...].astype(F32) * values_grad[...]
        owner = lax.broadcasted_iota(jnp.int32, (8, width), 1) // depth
        pick = jnp.where(owner == lax.broadcasted_iota(jnp.int32, (8, width), 0), 1.0, 0.0).astype(BF16)
        by_head = sum(dot(pick, part, 1, 1) for part in thirds(change))
        through = unstacked(dot(stacked(by_head), tri[...], 1, 1))
        row = lax.broadcasted_iota(jnp.int32, (8, 1), 0)
        beyond = jnp.zeros((8, 1), F32)
        for h in range(heads):
            part = slice(h * depth, (h + 1) * depth)
            end = before[part] * jnp.exp(down[rows - 1 : rows, h : h + 1]) + own_state[part, :]
            flow = jnp.sum(jnp.sum(end * state_grad[part, :], axis=0, keepdims=True), axis=1, keepdims=True)
            beyond = jnp.where(row == h, flow, beyond)
        decay_grad[...] = (through + beyond)[0:heads, :]

    extra = [finish_queries, finish_keys, finish_decays]
    for a in range(2):
        product(a, reach)
    for c in ORDER:
        for a in range(2):
            for way in range(2):
                if comes(way, 0, c):
                    hop(a, way, 0, c)
    for s in range(1, reach):
        for a in range(2):
            for way in range(2):
                product(a, block_of(a, way, s))
        if s > 1 and extra:
            extra.pop(0)()
        for c in ORDER:
            for a in range(2):
                for way in range(2):
                    if comes(way, s - 1, c):
                        axes[a][7][block_of(a, way, s), span(a, c), :] += landed(a, way, s - 1, c)
                    hop(a, way, s, c)
    for a in range(2):
        product(a, 0)
    for c in ORDER:
        for a in range(2):
            _, _, _, name_o, n_o, at_o, _, partial, _, block, last = axes[a]
            block[span(a, c), :] = partial[0, span(a, c), :] + landed(a, 0, reach - 1, c) + landed(a, 1, reach - 1, c)
            each = n_o // CHUNKS
            for j in range(c * each, (c + 1) * each):
                part = pl.ds(j * small, small)
                if j == 0:
                    last[0] = block[part, :]
                else:
                    pltpu.make_async_remote_copy(
                        src_ref=block.at[part], dst_ref=last.at[j], send_sem=last_send.at[a], recv_sem=last_recv.at[a],
                        device_id={name_o: lax.rem(at_o + j, n_o)}, device_id_type=MESH,
                    ).start()
    for work in extra:
        work()

    squares = jnp.zeros((small, pair), F32)
    for a in range(2):
        n_o, last = axes[a][4], axes[a][10]
        arrived(last.at[pl.ds(1, n_o - 1)], last_recv.at[a])
        done = last[0]
        for j in range(1, n_o):
            done += last[j]
        weight_grad[:, a * pair : (a + 1) * pair] = done
        squares += done * done
    ones = jnp.ones((8, pair), BF16)
    own_norms = sum(dot(ones, part, 1, 1) for part in thirds(squares))
    norm_out[...] = jnp.zeros_like(norm_out)
    norm_out[:, 0:small] = own_norms
    for j in range(1, nt):
        pltpu.make_async_remote_copy(
            src_ref=norm_out, dst_ref=norm_in.at[j], send_sem=norm_send, recv_sem=norm_recv,
            device_id={"tp": lax.rem(t + j, nt)}, device_id_type=MESH,
        ).start()
    if nt > 1:
        arrived(norm_in.at[pl.ds(1, nt - 1)], norm_recv)
    sums = norm_out[...]
    for j in range(1, nt):
        sums += norm_in[j]
    norms[...] = sums[0:1, 0:small]

    for i, buffer in enumerate((send_b, send_f, out_b, out_f)):
        arrived(first(buffer), scan_send.at[i])
    for a in range(2):
        n, n_o, partial, last = axes[a][1], axes[a][4], axes[a][7], axes[a][10]
        arrived(partial.at[pl.ds(0, n - 1)], ring_send.at[a])
        arrived(last.at[pl.ds(1, n_o - 1)], last_send.at[a])
    if nt > 1:
        arrived(norm_in.at[pl.ds(1, nt - 1)], norm_send)


def on_device(nz, ny, nt, block_input, value_weight, queries, key_rows, log_decay, out_grad):
    rows, model = block_input.shape
    width, heads, state = out_grad.shape[1], log_decay.shape[1], queries.shape[1]
    shards = nz * ny
    pair = 2 * (width // heads)
    reach = nz // 2
    tall_a, tall_b, small = model // nz, model // ny, model // shards
    vmem, dma = pltpu.VMEM, pltpu.SemaphoreType.DMA
    shape = jax.ShapeDtypeStruct
    scratch = [
        vmem((heads, rows), F32), vmem((rows, width), BF16), vmem((rows, state), BF16), vmem((rows, state), BF16),
        vmem((rows, model), BF16), vmem((model, width), BF16),
        vmem((rows, width), BF16), vmem((heads, rows, pair), BF16), vmem((heads, rows, pair), BF16),
        vmem((rows, width), F32), vmem((rows, width), F32), vmem((rows, width), BF16), vmem((rows, width), BF16),
        vmem((rows, rows), BF16), vmem((rows, 128), F32), vmem((8, rows), F32),
        vmem((shards, 8, state), F32), vmem((shards, 8, state), F32), vmem((shards, heads, state), F32), vmem((shards, heads, state), F32),
        vmem((shards, heads, state), F32), vmem((shards, heads, state), F32), vmem((shards, heads, state), F32), vmem((shards, heads, state), F32),
        vmem((width, state), F32), vmem((width, state), F32), vmem((rows, width), F32), vmem((rows, width), F32),
        vmem((rows, state), F32), vmem((rows, state), F32), vmem((rows, width), BF16),
        vmem((nz, tall_a, rows), BF16), vmem((ny, tall_b, rows), BF16), vmem((nz, tall_a, pair), F32), vmem((ny, tall_b, pair), F32),
        vmem((reach, tall_a, pair), F32), vmem((reach, tall_a, pair), F32), vmem((reach, tall_b, pair), F32), vmem((reach, tall_b, pair), F32),
        vmem((tall_a, pair), F32), vmem((tall_b, pair), F32), vmem((ny, small, pair), F32), vmem((nz, small, pair), F32),
        vmem((8, 128), F32), vmem((nt, 8, 128), F32),
        dma((5 + LOADS,)), dma((4,)), dma((4,)), dma((2,)), dma((4 * reach * CHUNKS,)), dma((2,)), dma((2,)), dma, dma,
    ]
    query_grad, key_grad, decay_grad, weight_grad, norms = pl.pallas_call(
        functools.partial(kernel, nz, ny, nt),
        out_shape=(
            shape((rows, state), F32), shape((rows, state), F32), shape((heads, rows), F32),
            shape((small, width), F32), shape((1, small), F32),
        ),
        in_specs=[pl.BlockSpec(memory_space=pl.ANY)] * 6,
        out_specs=(pl.BlockSpec(memory_space=pltpu.VMEM),) * 5,
        scratch_shapes=scratch,
        compiler_params=pltpu.CompilerParams(
            collective_id=0, has_side_effects=True, vmem_limit_bytes=56 * 1024 * 1024
        ),
    )(log_decay.T, out_grad, queries, key_rows, block_input, value_weight)
    return query_grad, key_grad, decay_grad.T, weight_grad, norms.reshape(small)


def solution(mesh):
    nz = ny = 8
    nt = mesh.shape["tp"]
    split = Mesh(mesh.devices.reshape(nz, ny, nt), ("sp_0", "sp_1", "tp"))
    return jax.shard_map(
        functools.partial(on_device, nz, ny, nt),
        mesh=split,
        in_specs=(P(SP, None), P(None, "tp"), P(SP, "tp"), P(SP, "tp"), P(SP, "tp"), P(SP, "tp")),
        out_specs=(P(SP, "tp"), P(SP, "tp"), P(SP, "tp"), P(SP, "tp"), P(SP)),
        check_vma=False,
    )
```

```python
import functools

import jax
import jax.numpy as jnp
from jax import lax
from jax.experimental import pallas as pl
from jax.experimental.pallas import tpu as pltpu
from jax.sharding import Mesh
from jax.sharding import PartitionSpec as P

SP = ("sp_0", "sp_1")
F32 = jnp.float32
BF16 = jnp.bfloat16
MESH = pl.DeviceIdType.MESH
LOADS = 4
CHUNKS = 8


def dot(a, b, a_dim, b_dim):
    return lax.dot_general(a, b, (((a_dim,), (b_dim,)), ((), ())), preferred_element_type=F32)


def thirds(x):
    high = x.astype(BF16)
    rest = x - high.astype(F32)
    middle = rest.astype(BF16)
    low = (rest - middle.astype(F32)).astype(BF16)
    return high, middle, low


def far_first(n):
    return sorted(range(n), key=lambda d: -min(d, n - d))


def per_piece(n):
    each = max(n // CHUNKS, 1)
    seen = [d // each for d in far_first(n)]
    return list(dict.fromkeys(seen))


def kernel(
    nz, ny, nt,
    decay_hbm, grad_hbm, query_hbm, key_hbm, input_hbm, weight_hbm,
    query_grad, key_grad, decay_grad, weight_grad, norms,
    decay, grad, query, key, block_in, weight,
    value, value_of, grad_of, rise, fall, grad_rise, value_fall, tri, down, across,
    logs, row_logs, scan_send_buf, scan_recv_buf, row_send, row_recv, scan_out, scan_in, beyond_rows,
    own_state, state_grad, before, values_grad, mixed, local_q, local_k, rounded,
    turned_a, turned_b, partial_a, partial_b, ring_ap, ring_am, ring_bp, ring_bm,
    block_a, block_b, last_a, last_b, norm_out, norm_in,
    load_sem, log_send, log_recv, row_send_sem, row_recv_sem, scan_send, scan_recv, ring_send, ring_recv, last_send, last_recv, norm_send, norm_recv,
):
    z, y, t = lax.axis_index("sp_0"), lax.axis_index("sp_1"), lax.axis_index("tp")
    shards = nz * ny
    me = z * ny + y
    rows, width = grad.shape
    heads = decay.shape[0]
    depth = width // heads
    pair = 2 * depth
    state = query.shape[1]
    piece = rows // LOADS

    loads = [
        pltpu.make_async_copy(decay_hbm, decay, load_sem.at[0]),
        pltpu.make_async_copy(grad_hbm, grad, load_sem.at[1]),
        pltpu.make_async_copy(query_hbm, query, load_sem.at[2]),
        pltpu.make_async_copy(weight_hbm, weight, load_sem.at[3]),
        pltpu.make_async_copy(key_hbm, key, load_sem.at[4]),
    ]
    for i in range(LOADS):
        part = pl.ds(i * piece, piece)
        loads.append(pltpu.make_async_copy(input_hbm.at[part], block_in.at[part], load_sem.at[5 + i]))
    for copy in loads:
        copy.start()

    barrier = pltpu.get_barrier_semaphore()

    lines = {"sp_0": (z, nz), "sp_1": (y, ny), "tp": (t, nt)}

    def others(name):
        at, n = lines[name]
        return [lax.rem(at + d, n) for d in far_first(n) if d]

    for name in lines:
        for other in others(name):
            pl.semaphore_signal(barrier, inc=1, device_id={name: other}, device_id_type=MESH)

    def along(name, source, target, send_sem, recv_sem):
        for other in others(name):
            pltpu.make_async_remote_copy(
                src_ref=source(other), dst_ref=target, send_sem=send_sem, recv_sem=recv_sem,
                device_id={name: other}, device_id_type=MESH,
            ).start()

    def arrived(buffer, sem):
        pltpu.make_async_copy(buffer, buffer, sem).wait()

    def all_but_one(buffer):
        return buffer.at[pl.ds(0, buffer.shape[0] - 1)]

    early = lax.broadcasted_iota(jnp.int32, (rows, rows), 0) <= lax.broadcasted_iota(jnp.int32, (rows, rows), 1)
    tri[...] = jnp.where(early, 1.0, 0.0).astype(BF16)

    def stacked(x):
        high, middle, low = thirds(x)
        return jnp.concatenate(
            [high.astype(F32), middle.astype(F32), low.astype(F32), jnp.zeros_like(x)], axis=0
        ).astype(BF16)

    def unstacked(x):
        return x[0:8] + x[8:16] + x[16:24]

    loads[0].wait()
    log8 = jnp.concatenate([decay[...]] * (8 // heads), axis=0)
    across[...] = unstacked(dot(stacked(log8), tri[...], 1, 0))
    down[...] = jnp.concatenate([across[...]] * 16, axis=0).T
    lane = lax.broadcasted_iota(jnp.int32, (rows, pair), 1)
    for h in range(0, heads, 2):
        cols = pl.ds(h * depth, pair)
        cum = jnp.where(
            lane < depth,
            jnp.broadcast_to(down[:, h : h + 1], (rows, pair)),
            jnp.broadcast_to(down[:, h + 1 : h + 2], (rows, pair)),
        )
        rise[:, cols] = jnp.exp(cum)
        fall[:, cols] = jnp.exp(cum[rows - 1 : rows, :] - cum)

    loads[1].wait()
    loads[2].wait()
    grad_rise[...] = (grad[...].astype(F32) * rise[...]).astype(BF16)
    tiles = depth // ny

    def pack(number, own):
        for g in range(ny):
            for h in range(heads):
                at = h * depth + g * tiles
                scan_send_buf[number, g, h] = own[at : at + tiles, :]

    pack(0, dot(grad_rise[...], query[...], 0, 0))
    logs[y] = down[rows - 1 : rows, :]

    def first_round(number):
        along(
            "sp_1", lambda other: scan_send_buf.at[number, other], scan_recv_buf.at[number, y],
            scan_send.at[number, 0], scan_recv.at[number, 0],
        )
        scan_recv_buf[number, y] = scan_send_buf[number, y]

    pl.semaphore_wait(barrier, nz - 1 + ny - 1 + nt - 1)
    along("sp_1", lambda other: logs.at[y], logs.at[y], log_send.at[0], log_recv.at[0])
    first_round(0)

    loads[3].wait()
    for i in range(LOADS):
        loads[5 + i].wait()
        part = pl.ds(i * piece, piece)
        value[part, :] = dot(block_in[part, :], weight[...], 1, 0).astype(BF16)
    loads[4].wait()
    value_fall[...] = (value[...].astype(F32) * fall[...]).astype(BF16)
    own_state[...] = dot(value_fall[...], key[...], 0, 0)
    pack(1, own_state[...])
    first_round(1)

    tall_a, tall_b = turned_a.shape[1], turned_b.shape[1]
    small = tall_a // ny
    for i in range(nz):
        turned_a[i] = block_in[:, i * tall_a : (i + 1) * tall_a].T
    for i in range(nz):
        for j in range(ny):
            turned_b[j, i * small : (i + 1) * small, :] = turned_a[i, j * small : (j + 1) * small, :]
    for h in range(heads):
        cols = pl.ds((h // 2) * pair, pair)
        mine = (lane < depth) if h % 2 == 0 else (lane >= depth)
        grad_of[h] = jnp.where(mine, grad[:, cols].astype(F32), 0.0).astype(BF16)
        value_of[h] = jnp.where(mine, value[:, cols].astype(F32), 0.0).astype(BF16)

    half = rows // 2
    causal = lax.broadcasted_iota(jnp.int32, (half, half), 0) >= lax.broadcasted_iota(jnp.int32, (half, half), 1)
    for late, early_block in ((0, 0), (1, 0), (1, 1)):
        to, of = pl.ds(late * half, half), pl.ds(early_block * half, half)
        scores = dot(query[to, :], key[of, :], 1, 1)
        score_grad = jnp.zeros((half, half), F32)
        for h0 in range(0, heads, 2):
            cols = pl.ds(h0 * depth, pair)
            for h in (h0, h0 + 1):
                gap = jnp.broadcast_to(down[to, h : h + 1], (half, half)) - jnp.broadcast_to(
                    across[h : h + 1, of], (half, half)
                )
                decayed = jnp.exp(jnp.minimum(gap, 0.0))
                if late == early_block:
                    decayed = jnp.where(causal, decayed, 0.0)
                score_grad += dot(grad_of[h, to, :], value[of, cols], 1, 1) * decayed
                weighted = (scores * decayed).astype(BF16)
                to_value = dot(weighted, grad_of[h, to, :], 0, 0)
                to_mixed = dot(weighted, value_of[h, of, :], 1, 0)
                if h == h0 and late == early_block:
                    if late == 0:
                        values_grad[of, cols] = to_value
                    else:
                        values_grad[of, cols] = to_value
                else:
                    values_grad[of, cols] += to_value
                if h == h0 and early_block == 0:
                    mixed[to, cols] = to_mixed
                else:
                    mixed[to, cols] += to_mixed
        score_grad = score_grad.astype(BF16)
        to_q = dot(score_grad, key[of, :], 1, 0)
        to_k = dot(score_grad, query[to, :], 0, 0)
        if early_block == 0:
            local_q[to, :] = to_q
        else:
            local_q[to, :] += to_q
        if late == early_block:
            local_k[of, :] = to_k
        else:
            local_k[of, :] += to_k

    arrived(all_but_one(logs), log_recv.at[0])
    line_logs = [logs[k] for k in range(ny)]
    row_logs[z] = sum(line_logs[1:], line_logs[0])
    along("sp_0", lambda other: row_logs.at[z], row_logs.at[z], log_send.at[1], log_recv.at[1])

    def splat(row):
        return [jnp.broadcast_to(row[:, h : h + 1], (tiles, state)) for h in range(heads)]

    factors = [splat(jnp.exp(row)) for row in line_logs]

    def steps(number, n):
        return list(range(n)) if number else list(reversed(range(n)))

    def row_copy(number, to, slot, sem):
        return pltpu.make_async_remote_copy(
            src_ref=row_send.at[number], dst_ref=row_recv.at[number, slot],
            send_sem=row_send_sem.at[number, sem], recv_sem=row_recv_sem.at[number, slot],
            device_id={"sp_0": to}, device_id_type=MESH,
        )

    def each_row(number, sent, sem):
        for k in range(nz):

            @pl.when(k > z if bool(number) == sent else k < z)
            def _():
                arrived(row_recv.at[number, k], sem.at[number, k])

    def line(number):
        arrived(all_but_one(scan_recv_buf.at[number]), scan_recv.at[number, 0])
        total = [jnp.zeros((tiles, state), F32) for _ in range(heads)]
        for k in steps(number, ny):
            for h in range(heads):
                scan_out[number, k, h] = total[h]
                total[h] = factors[k][h] * total[h] + scan_recv_buf[number, k, h]
        for h in range(heads):
            row_send[number, h] = total[h]
        for d in range(1, nz):
            other = z + d if number else z - d
            inside = other < nz if number else other >= 0

            @pl.when(inside)
            def _():
                row_copy(number, other, z, other).start()

    def line_factors(k):
        return splat(jnp.exp(row_logs[k]))

    def plane(number):
        each_row(number, False, row_recv_sem)
        total = [jnp.zeros((tiles, state), F32) for _ in range(heads)]
        for k in steps(number, nz):
            for h in range(heads):
                beyond_rows[k, h] = total[h]
                total[h] = whole_factors[k][h] * total[h] + row_recv[number, k, h]
        reaching = [beyond_rows[z, h] for h in range(heads)]
        for k in steps(number, ny):
            for h in range(heads):
                scan_out[number, k, h] += reaching[h]
                reaching[h] = factors[k][h] * reaching[h]
        scan_in[number, y] = scan_out[number, y]
        along(
            "sp_1", lambda other: scan_out.at[number, other], scan_in.at[number, y],
            scan_send.at[number, 2], scan_recv.at[number, 2],
        )

    def unpack(number, target):
        arrived(all_but_one(scan_in.at[number]), scan_recv.at[number, 2])
        for g in range(ny):
            for h in range(heads):
                at = h * depth + g * tiles
                target[at : at + tiles, :] = scan_in[number, g, h]

    line(0)
    arrived(all_but_one(row_logs), log_recv.at[1])
    whole_factors = [line_factors(k) for k in range(nz)]
    line(1)
    plane(0)
    plane(1)

    unpack(0, state_grad)
    state_grad_16 = state_grad[...].astype(BF16)
    values_grad[...] += fall[...] * dot(key[...], state_grad_16, 1, 1)
    rounded[...] = values_grad[...].astype(BF16)

    axes = (
        ("sp_0", nz, z, "sp_1", ny, y, turned_a, partial_a, (ring_ap, ring_am), block_a, last_a),
        ("sp_1", ny, y, "sp_0", nz, z, turned_b, partial_b, (ring_bp, ring_bm), block_b, last_b),
    )
    reach = ring_ap.shape[0]

    def product(a, r):
        _, n, at, _, n_o, at_o, turned, partial, _, _, _ = axes[a]
        block = dot(turned[lax.rem(at + r, n)], rounded[:, a * pair : (a + 1) * pair], 1, 0)
        for q in range(n_o):
            where = pl.multiple_of(lax.rem(q + n_o - at_o, n_o) * small, small)
            partial[r, pl.ds(where, small), :] = block[q * small : (q + 1) * small, :]

    def comes(way, s, c):
        return s > 0 or (c < CHUNKS // 2) == (way == 0)

    def slot(a, way, s, c):
        return ((a * 2 + way) * reach + s) * CHUNKS + c

    def span(a, c):
        tall = axes[a][7].shape[1] // CHUNKS
        return pl.ds(c * tall, tall)

    def block_of(a, way, s):
        n = axes[a][1]
        return reach - s if way == 0 else n - reach + s

    def hop(a, way, s, c):
        name, n, at, _, _, _, _, partial, ring, _, _ = axes[a]
        pltpu.make_async_remote_copy(
            src_ref=partial.at[block_of(a, way, s), span(a, c)], dst_ref=ring[way].at[s, span(a, c)],
            send_sem=ring_send.at[a], recv_sem=ring_recv.at[slot(a, way, s, c)],
            device_id={name: lax.rem(at + (1 if way == 0 else n - 1), n)}, device_id_type=MESH,
        ).start()

    def landed(a, way, s, c):
        arrived(axes[a][8][way].at[s, span(a, c)], ring_recv.at[slot(a, way, s, c)])
        return axes[a][8][way][s, span(a, c), :]

    def finish_queries():
        unpack(1, before)
        query_grad[...] = local_q[...] + dot(grad_rise[...], before[...].astype(BF16), 1, 0)

    def finish_keys():
        key_grad[...] = local_k[...] + dot(value_fall[...], state_grad[...].astype(BF16), 1, 0)

    def mixer_change():
        whole = mixed[...] + rise[...] * dot(query[...], before[...].astype(BF16), 1, 1)
        mixed[...] = grad[...].astype(F32) * whole - value[...].astype(F32) * values_grad[...]

    def finish_decays():
        owner = lax.broadcasted_iota(jnp.int32, (8, width), 1) // depth
        pick = jnp.where(owner == lax.broadcasted_iota(jnp.int32, (8, width), 0), 1.0, 0.0).astype(BF16)
        by_head = sum(dot(pick, part, 1, 1) for part in thirds(mixed[...]))
        through = unstacked(dot(stacked(by_head), tri[...], 1, 1))
        decay_grad[...] = through[0:heads, :]

    def add_beyond():
        row = lax.broadcasted_iota(jnp.int32, (heads, 1), 0)
        beyond = jnp.zeros((heads, 1), F32)
        for h in range(heads):
            part = slice(h * depth, (h + 1) * depth)
            end = before[part, :] * jnp.exp(down[rows - 1 : rows, h : h + 1]) + own_state[part, :]
            flow = jnp.sum(jnp.sum(end * state_grad[part, :], axis=0, keepdims=True), axis=1, keepdims=True)
            beyond = jnp.where(row == h, flow, beyond)
        decay_grad[...] += beyond

    def products(s):
        if s == reach:
            return [functools.partial(product, a, 0) for a in range(2)]
        return [functools.partial(product, a, block_of(a, way, s)) for a in range(2) for way in range(2)]

    gaps = [work for s in range(3, reach + 1) for work in products(s)]
    gaps += [finish_queries, finish_keys, mixer_change, finish_decays, add_beyond]
    order = per_piece(ny)
    for a in range(2):
        product(a, reach)
        for c in order:
            for way in range(2):
                if comes(way, 0, c):
                    hop(a, way, 0, c)
    for s in range(1, 3):
        for work in products(s):
            work()
    for s in range(1, reach):
        for i, c in enumerate(order):
            for a in range(2):
                for way in range(2):
                    if comes(way, s - 1, c):
                        axes[a][7][block_of(a, way, s), span(a, c), :] += landed(a, way, s - 1, c)
                    hop(a, way, s, c)
            if i % 2 and gaps:
                gaps.pop(0)()
    for c in order:
        for a in range(2):
            _, _, _, name_o, n_o, at_o, _, partial, _, block, last = axes[a]
            block[span(a, c), :] = partial[0, span(a, c), :] + landed(a, 0, reach - 1, c) + landed(a, 1, reach - 1, c)
            each = n_o // CHUNKS
            for j in range(c * each, (c + 1) * each):
                part = pl.ds(j * small, small)
                if j == 0:
                    last[0] = block[part, :]
                else:
                    pltpu.make_async_remote_copy(
                        src_ref=block.at[part], dst_ref=last.at[j], send_sem=last_send.at[a], recv_sem=last_recv.at[a],
                        device_id={name_o: lax.rem(at_o + j, n_o)}, device_id_type=MESH,
                    ).start()
    for work in gaps:
        work()

    squares = jnp.zeros((small, pair), F32)
    for a in range(2):
        n_o, last = axes[a][4], axes[a][10]
        arrived(last.at[pl.ds(1, n_o - 1)], last_recv.at[a])
        done = last[0]
        for j in range(1, n_o):
            done += last[j]
        weight_grad[:, a * pair : (a + 1) * pair] = done
        squares += done * done
    ones = jnp.ones((8, pair), BF16)
    own_norms = sum(dot(ones, part, 1, 1) for part in thirds(squares))
    norm_out[...] = jnp.zeros_like(norm_out)
    norm_out[:, 0:small] = own_norms
    for j in range(1, nt):
        pltpu.make_async_remote_copy(
            src_ref=norm_out, dst_ref=norm_in.at[j], send_sem=norm_send, recv_sem=norm_recv,
            device_id={"tp": lax.rem(t + j, nt)}, device_id_type=MESH,
        ).start()
    if nt > 1:
        arrived(norm_in.at[pl.ds(1, nt - 1)], norm_recv)
    sums = norm_out[...]
    for j in range(1, nt):
        sums += norm_in[j]
    norms[...] = sums[0:1, 0:small]

    arrived(all_but_one(logs), log_send.at[0])
    arrived(all_but_one(row_logs), log_send.at[1])
    for number in range(2):
        arrived(all_but_one(scan_send_buf.at[number]), scan_send.at[number, 0])
        each_row(number, True, row_send_sem)
        arrived(all_but_one(scan_out.at[number]), scan_send.at[number, 2])
    for a in range(2):
        n, n_o, partial, last = axes[a][1], axes[a][4], axes[a][7], axes[a][10]
        arrived(partial.at[pl.ds(0, n - 1)], ring_send.at[a])
        arrived(last.at[pl.ds(1, n_o - 1)], last_send.at[a])
    if nt > 1:
        arrived(norm_in.at[pl.ds(1, nt - 1)], norm_send)


def put_out(*refs):
    *sources, sems = refs
    count = len(sources) // 2
    copies = [pltpu.make_async_copy(sources[i], sources[count + i], sems.at[i]) for i in range(count)]
    for copy in copies:
        copy.start()
    for copy in copies:
        copy.wait()


def on_device(nz, ny, nt, block_input, value_weight, queries, key_rows, log_decay, out_grad):
    rows, model = block_input.shape
    width, heads, state = out_grad.shape[1], log_decay.shape[1], queries.shape[1]
    shards = nz * ny
    pair = 2 * (width // heads)
    reach = nz // 2
    tall_a, tall_b, small = model // nz, model // ny, model // shards
    tiles = width // heads // ny
    vmem, dma = pltpu.VMEM, pltpu.SemaphoreType.DMA
    shape = jax.ShapeDtypeStruct
    scratch = [
        vmem((heads, rows), F32), vmem((rows, width), BF16), vmem((rows, state), BF16), vmem((rows, state), BF16),
        vmem((rows, model), BF16), vmem((model, width), BF16),
        vmem((rows, width), BF16), vmem((heads, rows, pair), BF16), vmem((heads, rows, pair), BF16),
        vmem((rows, width), F32), vmem((rows, width), F32), vmem((rows, width), BF16), vmem((rows, width), BF16),
        vmem((rows, rows), BF16), vmem((rows, 128), F32), vmem((8, rows), F32),
        vmem((ny, 1, 128), F32), vmem((nz, 1, 128), F32),
        vmem((2, ny, heads, tiles, state), F32), vmem((2, ny, heads, tiles, state), F32),
        vmem((2, heads, tiles, state), F32), vmem((2, nz, heads, tiles, state), F32),
        vmem((2, ny, heads, tiles, state), F32), vmem((2, ny, heads, tiles, state), F32), vmem((nz, heads, tiles, state), F32),
        vmem((width, state), F32),
        vmem((width, state), F32), vmem((width, state), F32), vmem((rows, width), F32), vmem((rows, width), F32),
        vmem((rows, state), F32), vmem((rows, state), F32), vmem((rows, width), BF16),
        vmem((nz, tall_a, rows), BF16), vmem((ny, tall_b, rows), BF16), vmem((nz, tall_a, pair), F32), vmem((ny, tall_b, pair), F32),
        vmem((reach, tall_a, pair), F32), vmem((reach, tall_a, pair), F32), vmem((reach, tall_b, pair), F32), vmem((reach, tall_b, pair), F32),
        vmem((tall_a, pair), F32), vmem((tall_b, pair), F32), vmem((ny, small, pair), F32), vmem((nz, small, pair), F32),
        vmem((8, 128), F32), vmem((nt, 8, 128), F32),
        dma((5 + LOADS,)), dma((2,)), dma((2,)), dma((2, nz)), dma((2, nz)), dma((2, 3)), dma((2, 3)), dma((2,)), dma((4 * reach * CHUNKS,)), dma((2,)), dma((2,)), dma, dma,
    ]
    results = (
        ((rows, state), F32), ((rows, state), F32), ((heads, rows), F32), ((small, width), F32), ((1, small), F32)
    )
    kept = pl.pallas_call(
        functools.partial(kernel, nz, ny, nt),
        out_shape=tuple(vmem(*each) for each in results),
        in_specs=[pl.BlockSpec(memory_space=pl.ANY)] * 6,
        out_specs=(pl.BlockSpec(memory_space=pltpu.VMEM),) * 5,
        scratch_shapes=scratch,
        compiler_params=pltpu.CompilerParams(
            collective_id=0, has_side_effects=True, vmem_limit_bytes=56 * 1024 * 1024
        ),
    )(log_decay.T, out_grad, queries, key_rows, block_input, value_weight)
    query_grad, key_grad, decay_grad, weight_grad, norms = pl.pallas_call(
        put_out,
        out_shape=tuple(shape(*each) for each in results),
        in_specs=[pl.BlockSpec(memory_space=pltpu.VMEM)] * 5,
        out_specs=(pl.BlockSpec(memory_space=pl.ANY),) * 5,
        scratch_shapes=[dma((5,))],
    )(*(pltpu.with_memory_space_constraint(each, pltpu.VMEM) for each in kept))
    return query_grad, key_grad, decay_grad.T, weight_grad, norms.reshape(small)


def solution(mesh):
    nz = ny = 8
    nt = mesh.shape["tp"]
    split = Mesh(mesh.devices.reshape(nz, ny, nt), ("sp_0", "sp_1", "tp"))
    return jax.shard_map(
        functools.partial(on_device, nz, ny, nt),
        mesh=split,
        in_specs=(P(SP, None), P(None, "tp"), P(SP, "tp"), P(SP, "tp"), P(SP, "tp"), P(SP, "tp")),
        out_specs=(P(SP, "tp"), P(SP, "tp"), P(SP, "tp"), P(SP, "tp"), P(SP)),
        check_vma=False,
    )
```

```python
import functools

import jax
import jax.numpy as jnp
from jax import lax
from jax.experimental import pallas as pl
from jax.experimental.pallas import tpu as pltpu
from jax.sharding import Mesh
from jax.sharding import PartitionSpec as P

SP = ("sp_0", "sp_1")
F32 = jnp.float32
BF16 = jnp.bfloat16
MESH = pl.DeviceIdType.MESH
LOADS = 4
PARTS = 2
CHUNKS = 8


def dot(a, b, a_dim, b_dim):
    return lax.dot_general(a, b, (((a_dim,), (b_dim,)), ((), ())), preferred_element_type=F32)


def thirds(x):
    high = x.astype(BF16)
    rest = x - high.astype(F32)
    middle = rest.astype(BF16)
    low = (rest - middle.astype(F32)).astype(BF16)
    return high, middle, low


def far_first(n):
    return sorted(range(n), key=lambda d: -min(d, n - d))


def per_piece(n):
    each = max(n // CHUNKS, 1)
    seen = [d // each for d in far_first(n)]
    return list(dict.fromkeys(seen))


def kernel(
    nz, ny, nt,
    decay_hbm, grad_hbm, query_hbm, key_hbm, input_hbm, weight_hbm,
    query_grad, key_grad, decay_grad, weight_grad, norms,
    decay, grad, query, key, block_in, weight,
    value, value_of, grad_of, rise, fall, grad_rise, value_fall, tri, down, across,
    logs, row_logs, scan_send_buf, scan_recv_buf, row_send, row_recv, scan_out, scan_in, beyond_rows,
    own_state, state_grad, before, values_grad, mixed, local_q, local_k, rounded,
    turned_a, turned_b, partial_a, partial_b, ring_ap, ring_am, ring_bp, ring_bm,
    block_a, block_b, last_a, last_b, norm_out, norm_in,
    load_sem, log_send, log_recv, row_send_sem, row_recv_sem, scan_send, scan_recv, ring_send, ring_recv, last_send, last_recv, norm_send, norm_recv,
):
    z, y, t = lax.axis_index("sp_0"), lax.axis_index("sp_1"), lax.axis_index("tp")
    shards = nz * ny
    me = z * ny + y
    rows, width = grad.shape
    heads = decay.shape[0]
    depth = width // heads
    pair = 2 * depth
    state = query.shape[1]
    piece = rows // LOADS

    loads = [
        pltpu.make_async_copy(decay_hbm, decay, load_sem.at[0]),
        pltpu.make_async_copy(grad_hbm, grad, load_sem.at[1]),
        pltpu.make_async_copy(query_hbm, query, load_sem.at[2]),
        pltpu.make_async_copy(weight_hbm, weight, load_sem.at[3]),
        pltpu.make_async_copy(key_hbm, key, load_sem.at[4]),
    ]
    for i in range(LOADS):
        part = pl.ds(i * piece, piece)
        loads.append(pltpu.make_async_copy(input_hbm.at[part], block_in.at[part], load_sem.at[5 + i]))
    for copy in loads:
        copy.start()

    barrier = pltpu.get_barrier_semaphore()

    lines = {"sp_0": (z, nz), "sp_1": (y, ny), "tp": (t, nt)}

    def others(name):
        at, n = lines[name]
        return [lax.rem(at + d, n) for d in far_first(n) if d]

    for name in lines:
        for other in others(name):
            pl.semaphore_signal(barrier, inc=1, device_id={name: other}, device_id_type=MESH)

    def along(name, source, target, send_sem, recv_sem):
        for other in others(name):
            pltpu.make_async_remote_copy(
                src_ref=source(other), dst_ref=target, send_sem=send_sem, recv_sem=recv_sem,
                device_id={name: other}, device_id_type=MESH,
            ).start()

    def arrived(buffer, sem):
        pltpu.make_async_copy(buffer, buffer, sem).wait()

    def all_but_one(buffer):
        return buffer.at[pl.ds(0, buffer.shape[0] - 1)]

    early = lax.broadcasted_iota(jnp.int32, (rows, rows), 0) <= lax.broadcasted_iota(jnp.int32, (rows, rows), 1)
    tri[...] = jnp.where(early, 1.0, 0.0).astype(BF16)

    def stacked(x):
        high, middle, low = thirds(x)
        return jnp.concatenate(
            [high.astype(F32), middle.astype(F32), low.astype(F32), jnp.zeros_like(x)], axis=0
        ).astype(BF16)

    def unstacked(x):
        return x[0:8] + x[8:16] + x[16:24]

    loads[0].wait()
    log8 = jnp.concatenate([decay[...]] * (8 // heads), axis=0)
    across[...] = unstacked(dot(stacked(log8), tri[...], 1, 0))
    down[...] = jnp.concatenate([across[...]] * 16, axis=0).T
    lane = lax.broadcasted_iota(jnp.int32, (rows, pair), 1)
    for h in range(0, heads, 2):
        cols = pl.ds(h * depth, pair)
        cum = jnp.where(
            lane < depth,
            jnp.broadcast_to(down[:, h : h + 1], (rows, pair)),
            jnp.broadcast_to(down[:, h + 1 : h + 2], (rows, pair)),
        )
        rise[:, cols] = jnp.exp(cum)
        fall[:, cols] = jnp.exp(cum[rows - 1 : rows, :] - cum)

    loads[1].wait()
    loads[2].wait()
    grad_rise[...] = (grad[...].astype(F32) * rise[...]).astype(BF16)
    tiles = depth // ny

    group = heads // PARTS

    def pack(number, own):
        for g in range(ny):
            for h in range(heads):
                at = h * depth + g * tiles
                scan_send_buf[number, h // group, g, h % group] = own[at : at + tiles, :]

    pack(0, dot(grad_rise[...], query[...], 0, 0))
    logs[y] = down[rows - 1 : rows, :]

    def first_round(number):
        for p in range(PARTS):
            along(
                "sp_1", lambda other: scan_send_buf.at[number, p, other], scan_recv_buf.at[number, p, y],
                scan_send.at[number, 0, p], scan_recv.at[number, 0, p],
            )
            scan_recv_buf[number, p, y] = scan_send_buf[number, p, y]

    pl.semaphore_wait(barrier, nz - 1 + ny - 1 + nt - 1)
    along("sp_1", lambda other: logs.at[y], logs.at[y], log_send.at[0], log_recv.at[0])
    first_round(0)

    loads[3].wait()
    for i in range(LOADS):
        loads[5 + i].wait()
        part = pl.ds(i * piece, piece)
        value[part, :] = dot(block_in[part, :], weight[...], 1, 0).astype(BF16)
    loads[4].wait()
    value_fall[...] = (value[...].astype(F32) * fall[...]).astype(BF16)
    own_state[...] = dot(value_fall[...], key[...], 0, 0)
    pack(1, own_state[...])
    first_round(1)

    tall_a, tall_b = turned_a.shape[1], turned_b.shape[1]
    small = tall_a // ny
    for i in range(nz):
        turned_a[i] = block_in[:, i * tall_a : (i + 1) * tall_a].T
    for i in range(nz):
        for j in range(ny):
            turned_b[j, i * small : (i + 1) * small, :] = turned_a[i, j * small : (j + 1) * small, :]
    for h in range(heads):
        cols = pl.ds((h // 2) * pair, pair)
        mine = (lane < depth) if h % 2 == 0 else (lane >= depth)
        grad_of[h] = jnp.where(mine, grad[:, cols].astype(F32), 0.0).astype(BF16)
        value_of[h] = jnp.where(mine, value[:, cols].astype(F32), 0.0).astype(BF16)

    arrived(all_but_one(logs), log_recv.at[0])
    line_logs = [logs[k] for k in range(ny)]
    row_logs[z] = sum(line_logs[1:], line_logs[0])
    along("sp_0", lambda other: row_logs.at[z], row_logs.at[z], log_send.at[1], log_recv.at[1])

    def splat(row):
        return [jnp.broadcast_to(row[:, h : h + 1], (tiles, state)) for h in range(heads)]

    factors = [splat(jnp.exp(row)) for row in line_logs]

    def steps(number, n):
        return list(range(n)) if number else list(reversed(range(n)))

    def row_copy(number, p, to, slot, sem):
        return pltpu.make_async_remote_copy(
            src_ref=row_send.at[number, p], dst_ref=row_recv.at[number, p, slot],
            send_sem=row_send_sem.at[number, p, sem], recv_sem=row_recv_sem.at[number, p, slot],
            device_id={"sp_0": to}, device_id_type=MESH,
        )

    def each_row(number, p, sent, sem):
        for k in range(nz):

            @pl.when(k > z if bool(number) == sent else k < z)
            def _():
                arrived(row_recv.at[number, p, k], sem.at[number, p, k])

    def line(number, p):
        arrived(all_but_one(scan_recv_buf.at[number, p]), scan_recv.at[number, 0, p])
        total = [jnp.zeros((tiles, state), F32) for _ in range(group)]
        for k in steps(number, ny):
            for h in range(group):
                scan_out[number, p, k, h] = total[h]
                total[h] = factors[k][p * group + h] * total[h] + scan_recv_buf[number, p, k, h]
        for h in range(group):
            row_send[number, p, h] = total[h]
        for d in range(1, nz):
            other = z + d if number else z - d
            inside = other < nz if number else other >= 0

            @pl.when(inside)
            def _():
                row_copy(number, p, other, z, other).start()

    def line_factors(k):
        return splat(jnp.exp(row_logs[k]))

    def plane(number, p):
        each_row(number, p, False, row_recv_sem)
        total = [jnp.zeros((tiles, state), F32) for _ in range(group)]
        for k in steps(number, nz):
            for h in range(group):
                beyond_rows[number, p, k, h] = total[h]
                total[h] = whole_factors[k][p * group + h] * total[h] + row_recv[number, p, k, h]
        reaching = [beyond_rows[number, p, z, h] for h in range(group)]
        for k in steps(number, ny):
            for h in range(group):
                scan_out[number, p, k, h] += reaching[h]
                reaching[h] = factors[k][p * group + h] * reaching[h]
        scan_in[number, p, y] = scan_out[number, p, y]
        along(
            "sp_1", lambda other: scan_out.at[number, p, other], scan_in.at[number, p, y],
            scan_send.at[number, 1, p], scan_recv.at[number, 1, p],
        )

    def unpack(number, p, target):
        arrived(all_but_one(scan_in.at[number, p]), scan_recv.at[number, 1, p])
        for g in range(ny):
            for h in range(group):
                at = (p * group + h) * depth + g * tiles
                target[at : at + tiles, :] = scan_in[number, p, g, h]

    for p in range(PARTS):
        line(0, p)

    half = rows // 2
    causal = lax.broadcasted_iota(jnp.int32, (half, half), 0) >= lax.broadcasted_iota(jnp.int32, (half, half), 1)
    for late, early_block in ((0, 0), (1, 0), (1, 1)):
        to, of = pl.ds(late * half, half), pl.ds(early_block * half, half)
        scores = dot(query[to, :], key[of, :], 1, 1)
        score_grad = jnp.zeros((half, half), F32)
        for h0 in range(0, heads, 2):
            cols = pl.ds(h0 * depth, pair)
            for h in (h0, h0 + 1):
                gap = jnp.broadcast_to(down[to, h : h + 1], (half, half)) - jnp.broadcast_to(
                    across[h : h + 1, of], (half, half)
                )
                decayed = jnp.exp(jnp.minimum(gap, 0.0))
                if late == early_block:
                    decayed = jnp.where(causal, decayed, 0.0)
                score_grad += dot(grad_of[h, to, :], value[of, cols], 1, 1) * decayed
                weighted = (scores * decayed).astype(BF16)
                to_value = dot(weighted, grad_of[h, to, :], 0, 0)
                to_mixed = dot(weighted, value_of[h, of, :], 1, 0)
                if h == h0 and late == early_block:
                    if late == 0:
                        values_grad[of, cols] = to_value
                    else:
                        values_grad[of, cols] = to_value
                else:
                    values_grad[of, cols] += to_value
                if h == h0 and early_block == 0:
                    mixed[to, cols] = to_mixed
                else:
                    mixed[to, cols] += to_mixed
        score_grad = score_grad.astype(BF16)
        to_q = dot(score_grad, key[of, :], 1, 0)
        to_k = dot(score_grad, query[to, :], 0, 0)
        if early_block == 0:
            local_q[to, :] = to_q
        else:
            local_q[to, :] += to_q
        if late == early_block:
            local_k[of, :] = to_k
        else:
            local_k[of, :] += to_k

    arrived(all_but_one(row_logs), log_recv.at[1])
    whole_factors = [line_factors(k) for k in range(nz)]
    for p in range(PARTS):
        line(1, p)
    for p in range(PARTS):
        plane(0, p)

    def value_half(a):
        for p in range(a * PARTS // 2, (a + 1) * PARTS // 2):
            unpack(0, p, state_grad)
        cols = slice(a * pair, (a + 1) * pair)
        values_grad[:, cols] += fall[:, cols] * dot(key[...], state_grad[cols, :].astype(BF16), 1, 1)
        rounded[:, cols] = values_grad[:, cols].astype(BF16)

    axes = (
        ("sp_0", nz, z, "sp_1", ny, y, turned_a, partial_a, (ring_ap, ring_am), block_a, last_a),
        ("sp_1", ny, y, "sp_0", nz, z, turned_b, partial_b, (ring_bp, ring_bm), block_b, last_b),
    )
    reach = ring_ap.shape[0]

    def product(a, r):
        _, n, at, _, n_o, at_o, turned, partial, _, _, _ = axes[a]
        block = dot(turned[lax.rem(at + r, n)], rounded[:, a * pair : (a + 1) * pair], 1, 0)
        for q in range(n_o):
            where = pl.multiple_of(lax.rem(q + n_o - at_o, n_o) * small, small)
            partial[r, pl.ds(where, small), :] = block[q * small : (q + 1) * small, :]

    def comes(way, s, c):
        return s > 0 or (c < CHUNKS // 2) == (way == 0)

    def slot(a, way, s, c):
        return ((a * 2 + way) * reach + s) * CHUNKS + c

    def span(a, c):
        tall = axes[a][7].shape[1] // CHUNKS
        return pl.ds(c * tall, tall)

    def block_of(a, way, s):
        n = axes[a][1]
        return reach - s if way == 0 else n - reach + s

    def hop(a, way, s, c):
        name, n, at, _, _, _, _, partial, ring, _, _ = axes[a]
        pltpu.make_async_remote_copy(
            src_ref=partial.at[block_of(a, way, s), span(a, c)], dst_ref=ring[way].at[s, span(a, c)],
            send_sem=ring_send.at[a], recv_sem=ring_recv.at[slot(a, way, s, c)],
            device_id={name: lax.rem(at + (1 if way == 0 else n - 1), n)}, device_id_type=MESH,
        ).start()

    def landed(a, way, s, c):
        arrived(axes[a][8][way].at[s, span(a, c)], ring_recv.at[slot(a, way, s, c)])
        return axes[a][8][way][s, span(a, c), :]

    def finish_queries():
        for p in range(PARTS):
            unpack(1, p, before)
        query_grad[...] = local_q[...] + dot(grad_rise[...], before[...].astype(BF16), 1, 0)

    def finish_keys():
        key_grad[...] = local_k[...] + dot(value_fall[...], state_grad[...].astype(BF16), 1, 0)

    def mixer_change():
        whole = mixed[...] + rise[...] * dot(query[...], before[...].astype(BF16), 1, 1)
        mixed[...] = grad[...].astype(F32) * whole - value[...].astype(F32) * values_grad[...]

    def finish_decays():
        owner = lax.broadcasted_iota(jnp.int32, (8, width), 1) // depth
        pick = jnp.where(owner == lax.broadcasted_iota(jnp.int32, (8, width), 0), 1.0, 0.0).astype(BF16)
        by_head = sum(dot(pick, part, 1, 1) for part in thirds(mixed[...]))
        through = unstacked(dot(stacked(by_head), tri[...], 1, 1))
        decay_grad[...] = through[0:heads, :]

    def add_beyond():
        row = lax.broadcasted_iota(jnp.int32, (heads, 1), 0)
        beyond = jnp.zeros((heads, 1), F32)
        for h in range(heads):
            part = slice(h * depth, (h + 1) * depth)
            end = before[part, :] * jnp.exp(down[rows - 1 : rows, h : h + 1]) + own_state[part, :]
            flow = jnp.sum(jnp.sum(end * state_grad[part, :], axis=0, keepdims=True), axis=1, keepdims=True)
            beyond = jnp.where(row == h, flow, beyond)
        decay_grad[...] += beyond

    def products(s):
        for a in range(2):
            for way in range(2 if 0 < s < reach else 1):
                product(a, block_of(a, way, s) if s < reach else 0)

    order = per_piece(ny)
    for a in range(2):
        value_half(a)
        product(a, reach)
        for c in order:
            for way in range(2):
                if comes(way, 0, c):
                    hop(a, way, 0, c)
    products(1)
    if reach > 2:
        products(2)
    for p in range(PARTS):
        plane(1, p)
    for s in range(1, reach):
        for c in order:
            for a in range(2):
                for way in range(2):
                    if comes(way, s - 1, c):
                        axes[a][7][block_of(a, way, s), span(a, c), :] += landed(a, way, s - 1, c)
                    hop(a, way, s, c)
        if s + 2 <= reach:
            products(s + 2)
        elif reach == 2:
            products(2)
        if s == max(reach - 2, 1):
            finish_keys()
    finish_queries()
    for c in order:
        for a in range(2):
            _, _, _, name_o, n_o, at_o, _, partial, _, block, last = axes[a]
            block[span(a, c), :] = partial[0, span(a, c), :] + landed(a, 0, reach - 1, c) + landed(a, 1, reach - 1, c)
            each = n_o // CHUNKS
            for j in range(c * each, (c + 1) * each):
                part = pl.ds(j * small, small)
                if j == 0:
                    last[0] = block[part, :]
                else:
                    pltpu.make_async_remote_copy(
                        src_ref=block.at[part], dst_ref=last.at[j], send_sem=last_send.at[a], recv_sem=last_recv.at[a],
                        device_id={name_o: lax.rem(at_o + j, n_o)}, device_id_type=MESH,
                    ).start()
    mixer_change()
    finish_decays()
    add_beyond()

    squares = jnp.zeros((small, pair), F32)
    for a in range(2):
        n_o, last = axes[a][4], axes[a][10]
        arrived(last.at[pl.ds(1, n_o - 1)], last_recv.at[a])
        done = last[0]
        for j in range(1, n_o):
            done += last[j]
        weight_grad[:, a * pair : (a + 1) * pair] = done
        squares += done * done
    ones = jnp.ones((8, pair), BF16)
    own_norms = sum(dot(ones, part, 1, 1) for part in thirds(squares))
    norm_out[...] = jnp.zeros_like(norm_out)
    norm_out[:, 0:small] = own_norms
    for j in range(1, nt):
        pltpu.make_async_remote_copy(
            src_ref=norm_out, dst_ref=norm_in.at[j], send_sem=norm_send, recv_sem=norm_recv,
            device_id={"tp": lax.rem(t + j, nt)}, device_id_type=MESH,
        ).start()
    if nt > 1:
        arrived(norm_in.at[pl.ds(1, nt - 1)], norm_recv)
    sums = norm_out[...]
    for j in range(1, nt):
        sums += norm_in[j]
    norms[...] = sums[0:1, 0:small]

    arrived(all_but_one(logs), log_send.at[0])
    arrived(all_but_one(row_logs), log_send.at[1])
    for number in range(2):
        for p in range(PARTS):
            arrived(all_but_one(scan_send_buf.at[number, p]), scan_send.at[number, 0, p])
            each_row(number, p, True, row_send_sem)
            arrived(all_but_one(scan_out.at[number, p]), scan_send.at[number, 1, p])
    for a in range(2):
        n, n_o, partial, last = axes[a][1], axes[a][4], axes[a][7], axes[a][10]
        arrived(partial.at[pl.ds(0, n - 1)], ring_send.at[a])
        arrived(last.at[pl.ds(1, n_o - 1)], last_send.at[a])
    if nt > 1:
        arrived(norm_in.at[pl.ds(1, nt - 1)], norm_send)


def put_out(*refs):
    *sources, sems = refs
    count = len(sources) // 2
    copies = [pltpu.make_async_copy(sources[i], sources[count + i], sems.at[i]) for i in range(count)]
    for copy in copies:
        copy.start()
    for copy in copies:
        copy.wait()


def on_device(nz, ny, nt, block_input, value_weight, queries, key_rows, log_decay, out_grad):
    rows, model = block_input.shape
    width, heads, state = out_grad.shape[1], log_decay.shape[1], queries.shape[1]
    shards = nz * ny
    pair = 2 * (width // heads)
    reach = nz // 2
    tall_a, tall_b, small = model // nz, model // ny, model // shards
    tiles, group = width // heads // ny, heads // PARTS
    vmem, dma = pltpu.VMEM, pltpu.SemaphoreType.DMA
    shape = jax.ShapeDtypeStruct
    scratch = [
        vmem((heads, rows), F32), vmem((rows, width), BF16), vmem((rows, state), BF16), vmem((rows, state), BF16),
        vmem((rows, model), BF16), vmem((model, width), BF16),
        vmem((rows, width), BF16), vmem((heads, rows, pair), BF16), vmem((heads, rows, pair), BF16),
        vmem((rows, width), F32), vmem((rows, width), F32), vmem((rows, width), BF16), vmem((rows, width), BF16),
        vmem((rows, rows), BF16), vmem((rows, 128), F32), vmem((8, rows), F32),
        vmem((ny, 1, 128), F32), vmem((nz, 1, 128), F32),
        vmem((2, PARTS, ny, group, tiles, state), F32), vmem((2, PARTS, ny, group, tiles, state), F32),
        vmem((2, PARTS, group, tiles, state), F32), vmem((2, PARTS, nz, group, tiles, state), F32),
        vmem((2, PARTS, ny, group, tiles, state), F32), vmem((2, PARTS, ny, group, tiles, state), F32),
        vmem((2, PARTS, nz, group, tiles, state), F32),
        vmem((width, state), F32),
        vmem((width, state), F32), vmem((width, state), F32), vmem((rows, width), F32), vmem((rows, width), F32),
        vmem((rows, state), F32), vmem((rows, state), F32), vmem((rows, width), BF16),
        vmem((nz, tall_a, rows), BF16), vmem((ny, tall_b, rows), BF16), vmem((nz, tall_a, pair), F32), vmem((ny, tall_b, pair), F32),
        vmem((reach, tall_a, pair), F32), vmem((reach, tall_a, pair), F32), vmem((reach, tall_b, pair), F32), vmem((reach, tall_b, pair), F32),
        vmem((tall_a, pair), F32), vmem((tall_b, pair), F32), vmem((ny, small, pair), F32), vmem((nz, small, pair), F32),
        vmem((8, 128), F32), vmem((nt, 8, 128), F32),
        dma((5 + LOADS,)), dma((2,)), dma((2,)), dma((2, PARTS, nz)), dma((2, PARTS, nz)), dma((2, 2, PARTS)), dma((2, 2, PARTS)), dma((2,)), dma((4 * reach * CHUNKS,)), dma((2,)), dma((2,)), dma, dma,
    ]
    results = (
        ((rows, state), F32), ((rows, state), F32), ((heads, rows), F32), ((small, width), F32), ((1, small), F32)
    )
    kept = pl.pallas_call(
        functools.partial(kernel, nz, ny, nt),
        out_shape=tuple(vmem(*each) for each in results),
        in_specs=[pl.BlockSpec(memory_space=pl.ANY)] * 6,
        out_specs=(pl.BlockSpec(memory_space=pltpu.VMEM),) * 5,
        scratch_shapes=scratch,
        compiler_params=pltpu.CompilerParams(
            collective_id=0, has_side_effects=True, vmem_limit_bytes=56 * 1024 * 1024
        ),
    )(log_decay.T, out_grad, queries, key_rows, block_input, value_weight)
    query_grad, key_grad, decay_grad, weight_grad, norms = pl.pallas_call(
        put_out,
        out_shape=tuple(shape(*each) for each in results),
        in_specs=[pl.BlockSpec(memory_space=pltpu.VMEM)] * 5,
        out_specs=(pl.BlockSpec(memory_space=pl.ANY),) * 5,
        scratch_shapes=[dma((5,))],
    )(*(pltpu.with_memory_space_constraint(each, pltpu.VMEM) for each in kept))
    return query_grad, key_grad, decay_grad.T, weight_grad, norms.reshape(small)


def solution(mesh):
    nz = ny = 8
    nt = mesh.shape["tp"]
    split = Mesh(mesh.devices.reshape(nz, ny, nt), ("sp_0", "sp_1", "tp"))
    return jax.shard_map(
        functools.partial(on_device, nz, ny, nt),
        mesh=split,
        in_specs=(P(SP, None), P(None, "tp"), P(SP, "tp"), P(SP, "tp"), P(SP, "tp"), P(SP, "tp")),
        out_specs=(P(SP, "tp"), P(SP, "tp"), P(SP, "tp"), P(SP, "tp"), P(SP)),
        check_vma=False,
    )
```

```python
import functools

import jax
import jax.numpy as jnp
from jax import lax
from jax.experimental import pallas as pl
from jax.experimental.pallas import tpu as pltpu
from jax.sharding import Mesh
from jax.sharding import PartitionSpec as P

SP = ("sp_0", "sp_1")
F32 = jnp.float32
BF16 = jnp.bfloat16
MESH = pl.DeviceIdType.MESH
LOADS = 4
PARTS = 2
CHUNKS = 8


def dot(a, b, a_dim, b_dim):
    return lax.dot_general(a, b, (((a_dim,), (b_dim,)), ((), ())), preferred_element_type=F32)


def thirds(x):
    high = x.astype(BF16)
    rest = x - high.astype(F32)
    middle = rest.astype(BF16)
    low = (rest - middle.astype(F32)).astype(BF16)
    return high, middle, low


def far_first(n):
    return sorted(range(n), key=lambda d: -min(d, n - d))


def per_piece(n):
    each = max(n // CHUNKS, 1)
    seen = [d // each for d in far_first(n)]
    return list(dict.fromkeys(seen))


def kernel(
    nz, ny, nt,
    decay_hbm, grad_hbm, query_hbm, key_hbm, input_hbm, weight_hbm,
    query_grad, key_grad, decay_grad, weight_grad, norms,
    decay, grad, query, key, block_in, weight,
    value, value_of, grad_of, rise, fall, grad_rise, value_fall, tri, down, across,
    logs, row_logs, scan_send_buf, scan_recv_buf, row_send, row_recv, scan_out, scan_in, beyond_rows,
    own_state, state_grad, before, values_grad, mixed, local_q, local_k, rounded,
    turned_a, turned_b, partial_a, partial_b, ring_ap, ring_am, ring_bp, ring_bm,
    block_a, block_b, last_a, last_b, norm_out, norm_in,
    load_sem, log_send, log_recv, row_send_sem, row_recv_sem, scan_send, scan_recv, ring_send, ring_recv, last_send, last_recv, norm_send, norm_recv,
):
    z, y, t = lax.axis_index("sp_0"), lax.axis_index("sp_1"), lax.axis_index("tp")
    shards = nz * ny
    me = z * ny + y
    rows, width = grad.shape
    heads = decay.shape[0]
    depth = width // heads
    pair = 2 * depth
    state = query.shape[1]
    piece = rows // LOADS

    loads = [
        pltpu.make_async_copy(decay_hbm, decay, load_sem.at[0]),
        pltpu.make_async_copy(grad_hbm, grad, load_sem.at[1]),
        pltpu.make_async_copy(query_hbm, query, load_sem.at[2]),
        pltpu.make_async_copy(weight_hbm, weight, load_sem.at[3]),
        pltpu.make_async_copy(key_hbm, key, load_sem.at[4]),
    ]
    for i in range(LOADS):
        part = pl.ds(i * piece, piece)
        loads.append(pltpu.make_async_copy(input_hbm.at[part], block_in.at[part], load_sem.at[5 + i]))
    for copy in loads:
        copy.start()

    barrier = pltpu.get_barrier_semaphore()

    lines = {"sp_0": (z, nz), "sp_1": (y, ny), "tp": (t, nt)}

    def others(name):
        at, n = lines[name]
        return [lax.rem(at + d, n) for d in far_first(n) if d]

    for name in lines:
        for other in others(name):
            pl.semaphore_signal(barrier, inc=1, device_id={name: other}, device_id_type=MESH)

    def along(name, source, target, send_sem, recv_sem):
        for other in others(name):
            pltpu.make_async_remote_copy(
                src_ref=source(other), dst_ref=target, send_sem=send_sem, recv_sem=recv_sem,
                device_id={name: other}, device_id_type=MESH,
            ).start()

    def arrived(buffer, sem):
        pltpu.make_async_copy(buffer, buffer, sem).wait()

    def all_but_one(buffer):
        return buffer.at[pl.ds(0, buffer.shape[0] - 1)]

    early = lax.broadcasted_iota(jnp.int32, (rows, rows), 0) <= lax.broadcasted_iota(jnp.int32, (rows, rows), 1)
    tri[...] = jnp.where(early, 1.0, 0.0).astype(BF16)

    def stacked(x):
        high, middle, low = thirds(x)
        return jnp.concatenate(
            [high.astype(F32), middle.astype(F32), low.astype(F32), jnp.zeros_like(x)], axis=0
        ).astype(BF16)

    def unstacked(x):
        return x[0:8] + x[8:16] + x[16:24]

    loads[0].wait()
    log8 = jnp.concatenate([decay[...]] * (8 // heads), axis=0)
    across[...] = unstacked(dot(stacked(log8), tri[...], 1, 0))
    down[...] = jnp.concatenate([across[...]] * 16, axis=0).T
    lane = lax.broadcasted_iota(jnp.int32, (rows, pair), 1)
    for h in range(0, heads, 2):
        cols = pl.ds(h * depth, pair)
        cum = jnp.where(
            lane < depth,
            jnp.broadcast_to(down[:, h : h + 1], (rows, pair)),
            jnp.broadcast_to(down[:, h + 1 : h + 2], (rows, pair)),
        )
        rise[:, cols] = jnp.exp(cum)
        fall[:, cols] = jnp.exp(cum[rows - 1 : rows, :] - cum)

    loads[1].wait()
    loads[2].wait()
    grad_rise[...] = (grad[...].astype(F32) * rise[...]).astype(BF16)
    tiles = depth // ny

    group = heads // PARTS

    def pack(number, own):
        for g in range(ny):
            for h in range(heads):
                at = h * depth + g * tiles
                scan_send_buf[number, h // group, g, h % group] = own[at : at + tiles, :]

    pack(0, dot(grad_rise[...], query[...], 0, 0))
    logs[y] = down[rows - 1 : rows, :]

    def first_round(number):
        for p in range(PARTS):
            along(
                "sp_1", lambda other: scan_send_buf.at[number, p, other], scan_recv_buf.at[number, p, y],
                scan_send.at[number, 0, p], scan_recv.at[number, 0, p],
            )
            scan_recv_buf[number, p, y] = scan_send_buf[number, p, y]

    pl.semaphore_wait(barrier, nz - 1 + ny - 1 + nt - 1)
    along("sp_1", lambda other: logs.at[y], logs.at[y], log_send.at[0], log_recv.at[0])
    first_round(0)

    loads[3].wait()
    for i in range(LOADS):
        loads[5 + i].wait()
        part = pl.ds(i * piece, piece)
        value[part, :] = dot(block_in[part, :], weight[...], 1, 0).astype(BF16)
    loads[4].wait()
    value_fall[...] = (value[...].astype(F32) * fall[...]).astype(BF16)
    own_state[...] = dot(value_fall[...], key[...], 0, 0)
    pack(1, own_state[...])
    first_round(1)

    tall_a, tall_b = turned_a.shape[1], turned_b.shape[1]
    small = tall_a // ny
    for i in range(nz):
        turned_a[i] = block_in[:, i * tall_a : (i + 1) * tall_a].T
    for i in range(nz):
        for j in range(ny):
            turned_b[j, i * small : (i + 1) * small, :] = turned_a[i, j * small : (j + 1) * small, :]
    for h in range(heads):
        cols = pl.ds((h // 2) * pair, pair)
        mine = (lane < depth) if h % 2 == 0 else (lane >= depth)
        grad_of[h] = jnp.where(mine, grad[:, cols].astype(F32), 0.0).astype(BF16)
        value_of[h] = jnp.where(mine, value[:, cols].astype(F32), 0.0).astype(BF16)

    arrived(all_but_one(logs), log_recv.at[0])
    line_logs = [logs[k] for k in range(ny)]
    row_logs[z] = sum(line_logs[1:], line_logs[0])
    along("sp_0", lambda other: row_logs.at[z], row_logs.at[z], log_send.at[1], log_recv.at[1])

    def splat(row):
        return [jnp.broadcast_to(row[:, h : h + 1], (tiles, state)) for h in range(heads)]

    factors = [splat(jnp.exp(row)) for row in line_logs]

    def steps(number, n):
        return list(range(n)) if number else list(reversed(range(n)))

    def row_copy(number, p, to):
        return pltpu.make_async_remote_copy(
            src_ref=row_send.at[number, p], dst_ref=row_recv.at[number, p, z],
            send_sem=row_send_sem.at[number, p], recv_sem=row_recv_sem.at[number, p],
            device_id={"sp_0": to}, device_id_type=MESH,
        )

    def each_row(number, p, sent, sem):
        count = nz - 1 - z if bool(number) == sent else z
        for k in range(1, nz):

            @pl.when(count == k)
            def _():
                arrived(row_recv.at[number, p, pl.ds(0, k)], sem.at[number, p])

    def line(number, p):
        arrived(all_but_one(scan_recv_buf.at[number, p]), scan_recv.at[number, 0, p])
        total = [jnp.zeros((tiles, state), F32) for _ in range(group)]
        for k in steps(number, ny):
            for h in range(group):
                scan_out[number, p, k, h] = total[h]
                total[h] = factors[k][p * group + h] * total[h] + scan_recv_buf[number, p, k, h]
        for h in range(group):
            row_send[number, p, h] = total[h]
        for d in range(1, nz):
            other = z + d if number else z - d
            inside = other < nz if number else other >= 0

            @pl.when(inside)
            def _():
                row_copy(number, p, other).start()

    def line_factors(k):
        return splat(jnp.exp(row_logs[k]))

    def plane(number, p):
        each_row(number, p, False, row_recv_sem)
        total = [jnp.zeros((tiles, state), F32) for _ in range(group)]
        for k in steps(number, nz):
            for h in range(group):
                beyond_rows[number, p, k, h] = total[h]
                total[h] = whole_factors[k][p * group + h] * total[h] + row_recv[number, p, k, h]
        reaching = [beyond_rows[number, p, z, h] for h in range(group)]
        for k in steps(number, ny):
            for h in range(group):
                scan_out[number, p, k, h] += reaching[h]
                reaching[h] = factors[k][p * group + h] * reaching[h]
        scan_in[number, p, y] = scan_out[number, p, y]
        along(
            "sp_1", lambda other: scan_out.at[number, p, other], scan_in.at[number, p, y],
            scan_send.at[number, 1, p], scan_recv.at[number, 1, p],
        )

    def unpack(number, p, target):
        arrived(all_but_one(scan_in.at[number, p]), scan_recv.at[number, 1, p])
        for g in range(ny):
            for h in range(group):
                at = (p * group + h) * depth + g * tiles
                target[at : at + tiles, :] = scan_in[number, p, g, h]

    for p in range(PARTS):
        line(0, p)

    half = rows // 2
    causal = lax.broadcasted_iota(jnp.int32, (half, half), 0) >= lax.broadcasted_iota(jnp.int32, (half, half), 1)
    for late, early_block in ((0, 0), (1, 0), (1, 1)):
        to, of = pl.ds(late * half, half), pl.ds(early_block * half, half)
        scores = dot(query[to, :], key[of, :], 1, 1)
        score_grad = jnp.zeros((half, half), F32)
        for h0 in range(0, heads, 2):
            cols = pl.ds(h0 * depth, pair)
            for h in (h0, h0 + 1):
                gap = jnp.broadcast_to(down[to, h : h + 1], (half, half)) - jnp.broadcast_to(
                    across[h : h + 1, of], (half, half)
                )
                decayed = jnp.exp(jnp.minimum(gap, 0.0))
                if late == early_block:
                    decayed = jnp.where(causal, decayed, 0.0)
                score_grad += dot(grad_of[h, to, :], value[of, cols], 1, 1) * decayed
                weighted = (scores * decayed).astype(BF16)
                to_value = dot(weighted, grad_of[h, to, :], 0, 0)
                to_mixed = dot(weighted, value_of[h, of, :], 1, 0)
                if h == h0 and late == early_block:
                    if late == 0:
                        values_grad[of, cols] = to_value
                    else:
                        values_grad[of, cols] = to_value
                else:
                    values_grad[of, cols] += to_value
                if h == h0 and early_block == 0:
                    mixed[to, cols] = to_mixed
                else:
                    mixed[to, cols] += to_mixed
        score_grad = score_grad.astype(BF16)
        to_q = dot(score_grad, key[of, :], 1, 0)
        to_k = dot(score_grad, query[to, :], 0, 0)
        if early_block == 0:
            local_q[to, :] = to_q
        else:
            local_q[to, :] += to_q
        if late == early_block:
            local_k[of, :] = to_k
        else:
            local_k[of, :] += to_k

    arrived(all_but_one(row_logs), log_recv.at[1])
    whole_factors = [line_factors(k) for k in range(nz)]
    for p in range(PARTS):
        line(1, p)
    for p in range(PARTS):
        plane(0, p)

    def value_half(a):
        for p in range(a * PARTS // 2, (a + 1) * PARTS // 2):
            unpack(0, p, state_grad)
        cols = slice(a * pair, (a + 1) * pair)
        values_grad[:, cols] += fall[:, cols] * dot(key[...], state_grad[cols, :].astype(BF16), 1, 1)
        rounded[:, cols] = values_grad[:, cols].astype(BF16)

    axes = (
        ("sp_0", nz, z, "sp_1", ny, y, turned_a, partial_a, (ring_ap, ring_am), block_a, last_a),
        ("sp_1", ny, y, "sp_0", nz, z, turned_b, partial_b, (ring_bp, ring_bm), block_b, last_b),
    )
    reach = ring_ap.shape[0]

    def product(a, r):
        _, n, at, _, n_o, at_o, turned, partial, _, _, _ = axes[a]
        block = dot(turned[lax.rem(at + r, n)], rounded[:, a * pair : (a + 1) * pair], 1, 0)
        for q in range(n_o):
            where = pl.multiple_of(lax.rem(q + n_o - at_o, n_o) * small, small)
            partial[r, pl.ds(where, small), :] = block[q * small : (q + 1) * small, :]

    def comes(way, s, c):
        return s > 0 or (c < CHUNKS // 2) == (way == 0)

    def slot(s, c):
        return s * CHUNKS + c

    def span(a, c):
        tall = axes[a][7].shape[1] // CHUNKS
        return pl.ds(c * tall, tall)

    def block_of(a, way, s):
        n = axes[a][1]
        return reach - s if way == 0 else n - reach + s

    def hop(a, way, s, c):
        name, n, at, _, _, _, _, partial, ring, _, _ = axes[a]
        pltpu.make_async_remote_copy(
            src_ref=partial.at[block_of(a, way, s), span(a, c)], dst_ref=ring[way].at[s, span(a, c)],
            send_sem=ring_send.at[a], recv_sem=ring_recv.at[slot(s, c)],
            device_id={name: lax.rem(at + (1 if way == 0 else n - 1), n)}, device_id_type=MESH,
        ).start()

    def all_landed(s, c):
        flows = 2 * sum(comes(way, s, c) for way in range(2))
        arrived(axes[0][8][0].at[s, pl.ds(0, flows * (tall_a // CHUNKS))], ring_recv.at[slot(s, c)])

    def landed(a, way, s, c):
        return axes[a][8][way][s, span(a, c), :]

    def finish_queries():
        for p in range(PARTS):
            unpack(1, p, before)
        query_grad[...] = local_q[...] + dot(grad_rise[...], before[...].astype(BF16), 1, 0)

    def finish_keys():
        key_grad[...] = local_k[...] + dot(value_fall[...], state_grad[...].astype(BF16), 1, 0)

    def mixer_change():
        whole = mixed[...] + rise[...] * dot(query[...], before[...].astype(BF16), 1, 1)
        mixed[...] = grad[...].astype(F32) * whole - value[...].astype(F32) * values_grad[...]

    def finish_decays():
        owner = lax.broadcasted_iota(jnp.int32, (8, width), 1) // depth
        pick = jnp.where(owner == lax.broadcasted_iota(jnp.int32, (8, width), 0), 1.0, 0.0).astype(BF16)
        by_head = sum(dot(pick, part, 1, 1) for part in thirds(mixed[...]))
        through = unstacked(dot(stacked(by_head), tri[...], 1, 1))
        decay_grad[...] = through[0:heads, :]

    def add_beyond():
        row = lax.broadcasted_iota(jnp.int32, (heads, 1), 0)
        beyond = jnp.zeros((heads, 1), F32)
        for h in range(heads):
            part = slice(h * depth, (h + 1) * depth)
            end = before[part, :] * jnp.exp(down[rows - 1 : rows, h : h + 1]) + own_state[part, :]
            flow = jnp.sum(jnp.sum(end * state_grad[part, :], axis=0, keepdims=True), axis=1, keepdims=True)
            beyond = jnp.where(row == h, flow, beyond)
        decay_grad[...] += beyond

    def products(s):
        for a in range(2):
            for way in range(2 if 0 < s < reach else 1):
                product(a, block_of(a, way, s) if s < reach else 0)

    order = per_piece(ny)
    for a in range(2):
        value_half(a)
        product(a, reach)
        for c in order:
            for way in range(2):
                if comes(way, 0, c):
                    hop(a, way, 0, c)
    products(1)
    if reach > 2:
        products(2)
    for p in range(PARTS):
        plane(1, p)
    for s in range(1, reach):
        for c in order:
            all_landed(s - 1, c)
            for a in range(2):
                for way in range(2):
                    if comes(way, s - 1, c):
                        axes[a][7][block_of(a, way, s), span(a, c), :] += landed(a, way, s - 1, c)
                    hop(a, way, s, c)
        if s + 2 <= reach:
            products(s + 2)
        elif reach == 2:
            products(2)
        if s == max(reach - 2, 1):
            finish_keys()
    finish_queries()
    for c in order:
        all_landed(reach - 1, c)
        for a in range(2):
            _, _, _, name_o, n_o, at_o, _, partial, _, block, last = axes[a]
            block[span(a, c), :] = partial[0, span(a, c), :] + landed(a, 0, reach - 1, c) + landed(a, 1, reach - 1, c)
            each = n_o // CHUNKS
            for j in range(c * each, (c + 1) * each):
                part = pl.ds(j * small, small)
                if j == 0:
                    last[0] = block[part, :]
                else:
                    pltpu.make_async_remote_copy(
                        src_ref=block.at[part], dst_ref=last.at[j], send_sem=last_send.at[a], recv_sem=last_recv.at[a],
                        device_id={name_o: lax.rem(at_o + j, n_o)}, device_id_type=MESH,
                    ).start()
    mixer_change()
    finish_decays()
    add_beyond()

    squares = jnp.zeros((small, pair), F32)
    for a in range(2):
        n_o, last = axes[a][4], axes[a][10]
        arrived(last.at[pl.ds(1, n_o - 1)], last_recv.at[a])
        done = last[0]
        for j in range(1, n_o):
            done += last[j]
        weight_grad[:, a * pair : (a + 1) * pair] = done
        squares += done * done
    ones = jnp.ones((8, pair), BF16)
    own_norms = sum(dot(ones, part, 1, 1) for part in thirds(squares))
    norm_out[...] = jnp.zeros_like(norm_out)
    norm_out[:, 0:small] = own_norms
    for j in range(1, nt):
        pltpu.make_async_remote_copy(
            src_ref=norm_out, dst_ref=norm_in.at[j], send_sem=norm_send, recv_sem=norm_recv,
            device_id={"tp": lax.rem(t + j, nt)}, device_id_type=MESH,
        ).start()
    if nt > 1:
        arrived(norm_in.at[pl.ds(1, nt - 1)], norm_recv)
    sums = norm_out[...]
    for j in range(1, nt):
        sums += norm_in[j]
    norms[...] = sums[0:1, 0:small]

    arrived(all_but_one(logs), log_send.at[0])
    arrived(all_but_one(row_logs), log_send.at[1])
    for number in range(2):
        for p in range(PARTS):
            arrived(all_but_one(scan_send_buf.at[number, p]), scan_send.at[number, 0, p])
            each_row(number, p, True, row_send_sem)
            arrived(all_but_one(scan_out.at[number, p]), scan_send.at[number, 1, p])
    for a in range(2):
        n, n_o, partial, last = axes[a][1], axes[a][4], axes[a][7], axes[a][10]
        arrived(partial.at[pl.ds(0, n - 1)], ring_send.at[a])
        arrived(last.at[pl.ds(1, n_o - 1)], last_send.at[a])
    if nt > 1:
        arrived(norm_in.at[pl.ds(1, nt - 1)], norm_send)


def put_out(*refs):
    *sources, sems = refs
    count = len(sources) // 2
    copies = [pltpu.make_async_copy(sources[i], sources[count + i], sems.at[i]) for i in range(count)]
    for copy in copies:
        copy.start()
    for copy in copies:
        copy.wait()


def on_device(nz, ny, nt, block_input, value_weight, queries, key_rows, log_decay, out_grad):
    rows, model = block_input.shape
    width, heads, state = out_grad.shape[1], log_decay.shape[1], queries.shape[1]
    shards = nz * ny
    pair = 2 * (width // heads)
    reach = nz // 2
    tall_a, tall_b, small = model // nz, model // ny, model // shards
    tiles, group = width // heads // ny, heads // PARTS
    vmem, dma = pltpu.VMEM, pltpu.SemaphoreType.DMA
    shape = jax.ShapeDtypeStruct
    scratch = [
        vmem((heads, rows), F32), vmem((rows, width), BF16), vmem((rows, state), BF16), vmem((rows, state), BF16),
        vmem((rows, model), BF16), vmem((model, width), BF16),
        vmem((rows, width), BF16), vmem((heads, rows, pair), BF16), vmem((heads, rows, pair), BF16),
        vmem((rows, width), F32), vmem((rows, width), F32), vmem((rows, width), BF16), vmem((rows, width), BF16),
        vmem((rows, rows), BF16), vmem((rows, 128), F32), vmem((8, rows), F32),
        vmem((ny, 1, 128), F32), vmem((nz, 1, 128), F32),
        vmem((2, PARTS, ny, group, tiles, state), F32), vmem((2, PARTS, ny, group, tiles, state), F32),
        vmem((2, PARTS, group, tiles, state), F32), vmem((2, PARTS, nz, group, tiles, state), F32),
        vmem((2, PARTS, ny, group, tiles, state), F32), vmem((2, PARTS, ny, group, tiles, state), F32),
        vmem((2, PARTS, nz, group, tiles, state), F32),
        vmem((width, state), F32),
        vmem((width, state), F32), vmem((width, state), F32), vmem((rows, width), F32), vmem((rows, width), F32),
        vmem((rows, state), F32), vmem((rows, state), F32), vmem((rows, width), BF16),
        vmem((nz, tall_a, rows), BF16), vmem((ny, tall_b, rows), BF16), vmem((nz, tall_a, pair), F32), vmem((ny, tall_b, pair), F32),
        vmem((reach, tall_a, pair), F32), vmem((reach, tall_a, pair), F32), vmem((reach, tall_b, pair), F32), vmem((reach, tall_b, pair), F32),
        vmem((tall_a, pair), F32), vmem((tall_b, pair), F32), vmem((ny, small, pair), F32), vmem((nz, small, pair), F32),
        vmem((8, 128), F32), vmem((nt, 8, 128), F32),
        dma((5 + LOADS,)), dma((2,)), dma((2,)), dma((2, PARTS)), dma((2, PARTS)), dma((2, 2, PARTS)), dma((2, 2, PARTS)), dma((2,)), dma((reach * CHUNKS,)), dma((2,)), dma((2,)), dma, dma,
    ]
    results = (
        ((rows, state), F32), ((rows, state), F32), ((heads, rows), F32), ((small, width), F32), ((1, small), F32)
    )
    kept = pl.pallas_call(
        functools.partial(kernel, nz, ny, nt),
        out_shape=tuple(vmem(*each) for each in results),
        in_specs=[pl.BlockSpec(memory_space=pl.ANY)] * 6,
        out_specs=(pl.BlockSpec(memory_space=pltpu.VMEM),) * 5,
        scratch_shapes=scratch,
        compiler_params=pltpu.CompilerParams(
            collective_id=0, has_side_effects=True, vmem_limit_bytes=56 * 1024 * 1024
        ),
    )(log_decay.T, out_grad, queries, key_rows, block_input, value_weight)
    query_grad, key_grad, decay_grad, weight_grad, norms = pl.pallas_call(
        put_out,
        out_shape=tuple(shape(*each) for each in results),
        in_specs=[pl.BlockSpec(memory_space=pltpu.VMEM)] * 5,
        out_specs=(pl.BlockSpec(memory_space=pl.ANY),) * 5,
        scratch_shapes=[dma((5,))],
    )(*(pltpu.with_memory_space_constraint(each, pltpu.VMEM) for each in kept))
    return query_grad, key_grad, decay_grad.T, weight_grad, norms.reshape(small)


def solution(mesh):
    nz = ny = 8
    nt = mesh.shape["tp"]
    split = Mesh(mesh.devices.reshape(nz, ny, nt), ("sp_0", "sp_1", "tp"))
    return jax.shard_map(
        functools.partial(on_device, nz, ny, nt),
        mesh=split,
        in_specs=(P(SP, None), P(None, "tp"), P(SP, "tp"), P(SP, "tp"), P(SP, "tp"), P(SP, "tp")),
        out_specs=(P(SP, "tp"), P(SP, "tp"), P(SP, "tp"), P(SP, "tp"), P(SP)),
        check_vma=False,
    )
```

```python
import functools

import jax
import jax.numpy as jnp
from jax import lax
from jax.experimental import pallas as pl
from jax.experimental.pallas import tpu as pltpu
from jax.sharding import Mesh
from jax.sharding import PartitionSpec as P

SP = ("sp_0", "sp_1")
F32 = jnp.float32
BF16 = jnp.bfloat16
MESH = pl.DeviceIdType.MESH
LOADS = 4
PARTS = 2
CHUNKS = 8


def dot(a, b, a_dim, b_dim):
    return lax.dot_general(a, b, (((a_dim,), (b_dim,)), ((), ())), preferred_element_type=F32)


def thirds(x):
    high = x.astype(BF16)
    rest = x - high.astype(F32)
    middle = rest.astype(BF16)
    low = (rest - middle.astype(F32)).astype(BF16)
    return high, middle, low


def far_first(n):
    return sorted(range(n), key=lambda d: -min(d, n - d))


def per_piece(n):
    each = max(n // CHUNKS, 1)
    seen = [d // each for d in far_first(n)]
    return list(dict.fromkeys(seen))


def kernel(
    nz, ny, nt,
    decay_hbm, grad_hbm, query_hbm, key_hbm, input_hbm, weight_hbm,
    query_grad, key_grad, decay_grad, weight_grad, norms,
    decay, grad, query, key, block_in, weight,
    value, value_of, grad_of, rise, fall, grad_rise, value_fall, tri, down, across,
    logs, row_logs, scan_send_buf, scan_recv_buf, row_send, row_recv, scan_out, scan_in, beyond_rows,
    own_state, state_grad, before, values_grad, mixed, local_q, local_k, rounded,
    turned_a, turned_b, partial_a, partial_b, ring_ap, ring_am, ring_bp, ring_bm,
    block_a, block_b, last_a, last_b, norm_out, norm_in,
    load_sem, log_send, log_recv, row_send_sem, row_recv_sem, scan_send, scan_recv, ring_send, ring_recv, last_send, last_recv, norm_send, norm_recv,
):
    z, y, t = lax.axis_index("sp_0"), lax.axis_index("sp_1"), lax.axis_index("tp")
    shards = nz * ny
    me = z * ny + y
    rows, width = grad.shape
    heads = decay.shape[0]
    depth = width // heads
    pair = 2 * depth
    state = query.shape[1]
    piece = rows // LOADS

    loads = [
        pltpu.make_async_copy(decay_hbm, decay, load_sem.at[0]),
        pltpu.make_async_copy(grad_hbm, grad, load_sem.at[1]),
        pltpu.make_async_copy(query_hbm, query, load_sem.at[2]),
        pltpu.make_async_copy(weight_hbm, weight, load_sem.at[3]),
        pltpu.make_async_copy(key_hbm, key, load_sem.at[4]),
    ]
    for i in range(LOADS):
        part = pl.ds(i * piece, piece)
        loads.append(pltpu.make_async_copy(input_hbm.at[part], block_in.at[part], load_sem.at[5 + i]))
    for copy in loads:
        copy.start()

    barrier = pltpu.get_barrier_semaphore()

    lines = {"sp_0": (z, nz), "sp_1": (y, ny), "tp": (t, nt)}

    def others(name):
        at, n = lines[name]
        return [lax.rem(at + d, n) for d in far_first(n) if d]

    for name in lines:
        for other in others(name):
            pl.semaphore_signal(barrier, inc=1, device_id={name: other}, device_id_type=MESH)

    def along(name, source, target, send_sem, recv_sem):
        for other in others(name):
            pltpu.make_async_remote_copy(
                src_ref=source(other), dst_ref=target, send_sem=send_sem, recv_sem=recv_sem,
                device_id={name: other}, device_id_type=MESH,
            ).start()

    def arrived(buffer, sem):
        pltpu.make_async_copy(buffer, buffer, sem).wait()

    def all_but_one(buffer):
        return buffer.at[pl.ds(0, buffer.shape[0] - 1)]

    early = lax.broadcasted_iota(jnp.int32, (rows, rows), 0) <= lax.broadcasted_iota(jnp.int32, (rows, rows), 1)
    tri[...] = jnp.where(early, 1.0, 0.0).astype(BF16)

    def stacked(x):
        high, middle, low = thirds(x)
        return jnp.concatenate(
            [high.astype(F32), middle.astype(F32), low.astype(F32), jnp.zeros_like(x)], axis=0
        ).astype(BF16)

    def unstacked(x):
        return x[0:8] + x[8:16] + x[16:24]

    loads[0].wait()
    log8 = jnp.concatenate([decay[...]] * (8 // heads), axis=0)
    across[...] = unstacked(dot(stacked(log8), tri[...], 1, 0))
    down[...] = jnp.concatenate([across[...]] * 16, axis=0).T
    lane = lax.broadcasted_iota(jnp.int32, (rows, pair), 1)
    for h in range(0, heads, 2):
        cols = pl.ds(h * depth, pair)
        cum = jnp.where(
            lane < depth,
            jnp.broadcast_to(down[:, h : h + 1], (rows, pair)),
            jnp.broadcast_to(down[:, h + 1 : h + 2], (rows, pair)),
        )
        rise[:, cols] = jnp.exp(cum)
        fall[:, cols] = jnp.exp(cum[rows - 1 : rows, :] - cum)

    loads[1].wait()
    loads[2].wait()
    grad_rise[...] = (grad[...].astype(F32) * rise[...]).astype(BF16)
    tiles = depth // ny

    group = heads // PARTS

    def pack(number, own):
        for g in range(ny):
            for h in range(heads):
                at = h * depth + g * tiles
                scan_send_buf[number, h // group, g, h % group] = own[at : at + tiles, :]

    pack(0, dot(grad_rise[...], query[...], 0, 0))
    logs[y] = down[rows - 1 : rows, :]

    def first_round(number):
        for p in range(PARTS):
            along(
                "sp_1", lambda other: scan_send_buf.at[number, p, other], scan_recv_buf.at[number, p, y],
                scan_send.at[number, 0, p], scan_recv.at[number, 0, p],
            )
            scan_recv_buf[number, p, y] = scan_send_buf[number, p, y]

    pl.semaphore_wait(barrier, nz - 1 + ny - 1 + nt - 1)
    along("sp_1", lambda other: logs.at[y], logs.at[y], log_send.at[0], log_recv.at[0])
    first_round(0)

    loads[3].wait()
    for i in range(LOADS):
        loads[5 + i].wait()
        part = pl.ds(i * piece, piece)
        value[part, :] = dot(block_in[part, :], weight[...], 1, 0).astype(BF16)
    loads[4].wait()
    value_fall[...] = (value[...].astype(F32) * fall[...]).astype(BF16)
    own_state[...] = dot(value_fall[...], key[...], 0, 0)
    pack(1, own_state[...])
    first_round(1)

    tall_a, tall_b = turned_a.shape[1], turned_b.shape[1]
    small = tall_a // ny
    for i in range(nz):
        turned_a[i] = block_in[:, i * tall_a : (i + 1) * tall_a].T
    for i in range(nz):
        for j in range(ny):
            turned_b[j, i * small : (i + 1) * small, :] = turned_a[i, j * small : (j + 1) * small, :]
    for h in range(heads):
        cols = pl.ds((h // 2) * pair, pair)
        mine = (lane < depth) if h % 2 == 0 else (lane >= depth)
        grad_of[h] = jnp.where(mine, grad[:, cols].astype(F32), 0.0).astype(BF16)
        value_of[h] = jnp.where(mine, value[:, cols].astype(F32), 0.0).astype(BF16)

    arrived(all_but_one(logs), log_recv.at[0])
    line_logs = [logs[k] for k in range(ny)]
    row_logs[z] = sum(line_logs[1:], line_logs[0])
    along("sp_0", lambda other: row_logs.at[z], row_logs.at[z], log_send.at[1], log_recv.at[1])

    def splat(row):
        return [jnp.broadcast_to(row[:, h : h + 1], (tiles, state)) for h in range(heads)]

    factors = [splat(jnp.exp(row)) for row in line_logs]

    def steps(number, n):
        return list(range(n)) if number else list(reversed(range(n)))

    def row_copy(number, p, to):
        return pltpu.make_async_remote_copy(
            src_ref=row_send.at[number, p], dst_ref=row_recv.at[number, p, z],
            send_sem=row_send_sem.at[number, p], recv_sem=row_recv_sem.at[number, p],
            device_id={"sp_0": to}, device_id_type=MESH,
        )

    def each_row(number, p, sent, sem):
        count = nz - 1 - z if bool(number) == sent else z
        for k in range(1, nz):

            @pl.when(count == k)
            def _():
                arrived(row_recv.at[number, p, pl.ds(0, k)], sem.at[number, p])

    def line(number, p):
        arrived(all_but_one(scan_recv_buf.at[number, p]), scan_recv.at[number, 0, p])
        total = [jnp.zeros((tiles, state), F32) for _ in range(group)]
        for k in steps(number, ny):
            for h in range(group):
                scan_out[number, p, k, h] = total[h]
                total[h] = factors[k][p * group + h] * total[h] + scan_recv_buf[number, p, k, h]
        for h in range(group):
            row_send[number, p, h] = total[h]
        for d in range(1, nz):
            other = z + d if number else z - d
            inside = other < nz if number else other >= 0

            @pl.when(inside)
            def _():
                row_copy(number, p, other).start()

    def line_factors(k):
        return splat(jnp.exp(row_logs[k]))

    def plane(number, p):
        each_row(number, p, False, row_recv_sem)
        total = [jnp.zeros((tiles, state), F32) for _ in range(group)]
        for k in steps(number, nz):
            for h in range(group):
                beyond_rows[number, p, k, h] = total[h]
                total[h] = whole_factors[k][p * group + h] * total[h] + row_recv[number, p, k, h]
        reaching = [beyond_rows[number, p, z, h] for h in range(group)]
        for k in steps(number, ny):
            for h in range(group):
                scan_out[number, p, k, h] += reaching[h]
                reaching[h] = factors[k][p * group + h] * reaching[h]
        scan_in[number, p, y] = scan_out[number, p, y]
        along(
            "sp_1", lambda other: scan_out.at[number, p, other], scan_in.at[number, p, y],
            scan_send.at[number, 1, p], scan_recv.at[number, 1, p],
        )

    def unpack(number, p, target):
        arrived(all_but_one(scan_in.at[number, p]), scan_recv.at[number, 1, p])
        for g in range(ny):
            for h in range(group):
                at = (p * group + h) * depth + g * tiles
                target[at : at + tiles, :] = scan_in[number, p, g, h]

    for p in range(PARTS):
        line(0, p)

    half = rows // 2
    causal = lax.broadcasted_iota(jnp.int32, (half, half), 0) >= lax.broadcasted_iota(jnp.int32, (half, half), 1)
    for late, early_block in ((0, 0), (1, 0), (1, 1)):
        to, of = pl.ds(late * half, half), pl.ds(early_block * half, half)
        scores = dot(query[to, :], key[of, :], 1, 1)
        score_grad = jnp.zeros((half, half), F32)
        for h0 in range(0, heads, 2):
            cols = pl.ds(h0 * depth, pair)
            for h in (h0, h0 + 1):
                gap = jnp.broadcast_to(down[to, h : h + 1], (half, half)) - jnp.broadcast_to(
                    across[h : h + 1, of], (half, half)
                )
                decayed = jnp.exp(jnp.minimum(gap, 0.0))
                if late == early_block:
                    decayed = jnp.where(causal, decayed, 0.0)
                score_grad += dot(grad_of[h, to, :], value[of, cols], 1, 1) * decayed
                weighted = (scores * decayed).astype(BF16)
                to_value = dot(weighted, grad_of[h, to, :], 0, 0)
                to_mixed = dot(weighted, value_of[h, of, :], 1, 0)
                if h == h0 and late == early_block:
                    if late == 0:
                        values_grad[of, cols] = to_value
                    else:
                        values_grad[of, cols] = to_value
                else:
                    values_grad[of, cols] += to_value
                if h == h0 and early_block == 0:
                    mixed[to, cols] = to_mixed
                else:
                    mixed[to, cols] += to_mixed
        score_grad = score_grad.astype(BF16)
        to_q = dot(score_grad, key[of, :], 1, 0)
        to_k = dot(score_grad, query[to, :], 0, 0)
        if early_block == 0:
            local_q[to, :] = to_q
        else:
            local_q[to, :] += to_q
        if late == early_block:
            local_k[of, :] = to_k
        else:
            local_k[of, :] += to_k

    arrived(all_but_one(row_logs), log_recv.at[1])
    whole_factors = [line_factors(k) for k in range(nz)]
    for p in range(PARTS):
        line(1, p)
    for p in range(PARTS):
        plane(0, p)

    def value_half(a):
        for p in range(a * PARTS // 2, (a + 1) * PARTS // 2):
            unpack(0, p, state_grad)
        cols = slice(a * pair, (a + 1) * pair)
        values_grad[:, cols] += fall[:, cols] * dot(key[...], state_grad[cols, :].astype(BF16), 1, 1)
        rounded[:, cols] = values_grad[:, cols].astype(BF16)

    axes = (
        ("sp_0", nz, z, "sp_1", ny, y, turned_a, partial_a, (ring_ap, ring_am), block_a, last_a),
        ("sp_1", ny, y, "sp_0", nz, z, turned_b, partial_b, (ring_bp, ring_bm), block_b, last_b),
    )
    reach = ring_ap.shape[0]

    def product(a, r):
        _, n, at, _, n_o, at_o, turned, partial, _, _, _ = axes[a]
        block = dot(turned[lax.rem(at + r, n)], rounded[:, a * pair : (a + 1) * pair], 1, 0)
        for q in range(n_o):
            where = pl.multiple_of(lax.rem(q + n_o - at_o, n_o) * small, small)
            partial[r, pl.ds(where, small), :] = block[q * small : (q + 1) * small, :]

    def comes(way, s, c):
        return s > 0 or (c < CHUNKS // 2) == (way == 0)

    def slot(s, c):
        return s * CHUNKS + c

    def span(a, c):
        tall = axes[a][7].shape[1] // CHUNKS
        return pl.ds(c * tall, tall)

    def block_of(a, way, s):
        n = axes[a][1]
        return reach - s if way == 0 else n - reach + s

    def hop(a, way, s, c):
        name, n, at, _, _, _, _, partial, ring, _, _ = axes[a]
        pltpu.make_async_remote_copy(
            src_ref=partial.at[block_of(a, way, s), span(a, c)], dst_ref=ring[way].at[s, span(a, c)],
            send_sem=ring_send.at[a], recv_sem=ring_recv.at[slot(s, c)],
            device_id={name: lax.rem(at + (1 if way == 0 else n - 1), n)}, device_id_type=MESH,
        ).start()

    def all_landed(s, c):
        flows = 2 * sum(comes(way, s, c) for way in range(2))
        arrived(axes[0][8][0].at[s, pl.ds(0, flows * (tall_a // CHUNKS))], ring_recv.at[slot(s, c)])

    def landed(a, way, s, c):
        return axes[a][8][way][s, span(a, c), :]

    def finish_queries():
        for p in range(PARTS):
            unpack(1, p, before)
        query_grad[...] = local_q[...] + dot(grad_rise[...], before[...].astype(BF16), 1, 0)

    def finish_keys():
        key_grad[...] = local_k[...] + dot(value_fall[...], state_grad[...].astype(BF16), 1, 0)

    def mixer_change():
        whole = mixed[...] + rise[...] * dot(query[...], before[...].astype(BF16), 1, 1)
        mixed[...] = grad[...].astype(F32) * whole - value[...].astype(F32) * values_grad[...]

    def finish_decays():
        owner = lax.broadcasted_iota(jnp.int32, (8, width), 1) // depth
        pick = jnp.where(owner == lax.broadcasted_iota(jnp.int32, (8, width), 0), 1.0, 0.0).astype(BF16)
        by_head = sum(dot(pick, part, 1, 1) for part in thirds(mixed[...]))
        through = unstacked(dot(stacked(by_head), tri[...], 1, 1))
        decay_grad[...] = through[0:heads, :]

    def add_beyond():
        row = lax.broadcasted_iota(jnp.int32, (heads, 1), 0)
        beyond = jnp.zeros((heads, 1), F32)
        for h in range(heads):
            part = slice(h * depth, (h + 1) * depth)
            end = before[part, :] * jnp.exp(down[rows - 1 : rows, h : h + 1]) + own_state[part, :]
            flow = jnp.sum(jnp.sum(end * state_grad[part, :], axis=0, keepdims=True), axis=1, keepdims=True)
            beyond = jnp.where(row == h, flow, beyond)
        decay_grad[...] += beyond

    def products(s):
        for a in range(2):
            for way in range(2 if 0 < s < reach else 1):
                product(a, block_of(a, way, s) if s < reach else 0)

    order = per_piece(ny)
    for a in range(2):
        value_half(a)
        product(a, reach)
        for c in order:
            for way in range(2):
                if comes(way, 0, c):
                    hop(a, way, 0, c)
    products(1)
    if reach > 2:
        products(2)
    for p in range(PARTS):
        plane(1, p)
    for s in range(1, reach):
        for c in order:
            all_landed(s - 1, c)
            for a in range(2):
                for way in range(2):
                    if comes(way, s - 1, c):
                        axes[a][7][block_of(a, way, s), span(a, c), :] += landed(a, way, s - 1, c)
                    hop(a, way, s, c)
        if s + 2 <= reach:
            products(s + 2)
        elif reach == 2:
            products(2)
    for c in order:
        all_landed(reach - 1, c)
        for a in range(2):
            _, _, _, name_o, n_o, at_o, _, partial, _, block, last = axes[a]
            block[span(a, c), :] = partial[0, span(a, c), :] + landed(a, 0, reach - 1, c) + landed(a, 1, reach - 1, c)
            each = n_o // CHUNKS
            for j in range(c * each, (c + 1) * each):
                part = pl.ds(j * small, small)
                if j == 0:
                    last[0] = block[part, :]
                else:
                    pltpu.make_async_remote_copy(
                        src_ref=block.at[part], dst_ref=last.at[j], send_sem=last_send.at[a], recv_sem=last_recv.at[a],
                        device_id={name_o: lax.rem(at_o + j, n_o)}, device_id_type=MESH,
                    ).start()
    finish_keys()
    finish_queries()
    mixer_change()
    finish_decays()
    add_beyond()

    squares = jnp.zeros((small, pair), F32)
    for a in range(2):
        n_o, last = axes[a][4], axes[a][10]
        arrived(last.at[pl.ds(1, n_o - 1)], last_recv.at[a])
        done = last[0]
        for j in range(1, n_o):
            done += last[j]
        weight_grad[:, a * pair : (a + 1) * pair] = done
        squares += done * done
    ones = jnp.ones((8, pair), BF16)
    own_norms = sum(dot(ones, part, 1, 1) for part in thirds(squares))
    norm_out[...] = jnp.zeros_like(norm_out)
    norm_out[:, 0:small] = own_norms
    for j in range(1, nt):
        pltpu.make_async_remote_copy(
            src_ref=norm_out, dst_ref=norm_in.at[j], send_sem=norm_send, recv_sem=norm_recv,
            device_id={"tp": lax.rem(t + j, nt)}, device_id_type=MESH,
        ).start()
    if nt > 1:
        arrived(norm_in.at[pl.ds(1, nt - 1)], norm_recv)
    sums = norm_out[...]
    for j in range(1, nt):
        sums += norm_in[j]
    norms[...] = sums[0:1, 0:small]

    arrived(all_but_one(logs), log_send.at[0])
    arrived(all_but_one(row_logs), log_send.at[1])
    for number in range(2):
        for p in range(PARTS):
            arrived(all_but_one(scan_send_buf.at[number, p]), scan_send.at[number, 0, p])
            each_row(number, p, True, row_send_sem)
            arrived(all_but_one(scan_out.at[number, p]), scan_send.at[number, 1, p])
    for a in range(2):
        n, n_o, partial, last = axes[a][1], axes[a][4], axes[a][7], axes[a][10]
        arrived(partial.at[pl.ds(0, n - 1)], ring_send.at[a])
        arrived(last.at[pl.ds(1, n_o - 1)], last_send.at[a])
    if nt > 1:
        arrived(norm_in.at[pl.ds(1, nt - 1)], norm_send)


def put_out(*refs):
    *sources, sems = refs
    count = len(sources) // 2
    copies = [pltpu.make_async_copy(sources[i], sources[count + i], sems.at[i]) for i in range(count)]
    for copy in copies:
        copy.start()
    for copy in copies:
        copy.wait()


def on_device(nz, ny, nt, block_input, value_weight, queries, key_rows, log_decay, out_grad):
    rows, model = block_input.shape
    width, heads, state = out_grad.shape[1], log_decay.shape[1], queries.shape[1]
    shards = nz * ny
    pair = 2 * (width // heads)
    reach = nz // 2
    tall_a, tall_b, small = model // nz, model // ny, model // shards
    tiles, group = width // heads // ny, heads // PARTS
    vmem, dma = pltpu.VMEM, pltpu.SemaphoreType.DMA
    shape = jax.ShapeDtypeStruct
    scratch = [
        vmem((heads, rows), F32), vmem((rows, width), BF16), vmem((rows, state), BF16), vmem((rows, state), BF16),
        vmem((rows, model), BF16), vmem((model, width), BF16),
        vmem((rows, width), BF16), vmem((heads, rows, pair), BF16), vmem((heads, rows, pair), BF16),
        vmem((rows, width), F32), vmem((rows, width), F32), vmem((rows, width), BF16), vmem((rows, width), BF16),
        vmem((rows, rows), BF16), vmem((rows, 128), F32), vmem((8, rows), F32),
        vmem((ny, 1, 128), F32), vmem((nz, 1, 128), F32),
        vmem((2, PARTS, ny, group, tiles, state), F32), vmem((2, PARTS, ny, group, tiles, state), F32),
        vmem((2, PARTS, group, tiles, state), F32), vmem((2, PARTS, nz, group, tiles, state), F32),
        vmem((2, PARTS, ny, group, tiles, state), F32), vmem((2, PARTS, ny, group, tiles, state), F32),
        vmem((2, PARTS, nz, group, tiles, state), F32),
        vmem((width, state), F32),
        vmem((width, state), F32), vmem((width, state), F32), vmem((rows, width), F32), vmem((rows, width), F32),
        vmem((rows, state), F32), vmem((rows, state), F32), vmem((rows, width), BF16),
        vmem((nz, tall_a, rows), BF16), vmem((ny, tall_b, rows), BF16), vmem((nz, tall_a, pair), F32), vmem((ny, tall_b, pair), F32),
        vmem((reach, tall_a, pair), F32), vmem((reach, tall_a, pair), F32), vmem((reach, tall_b, pair), F32), vmem((reach, tall_b, pair), F32),
        vmem((tall_a, pair), F32), vmem((tall_b, pair), F32), vmem((ny, small, pair), F32), vmem((nz, small, pair), F32),
        vmem((8, 128), F32), vmem((nt, 8, 128), F32),
        dma((5 + LOADS,)), dma((2,)), dma((2,)), dma((2, PARTS)), dma((2, PARTS)), dma((2, 2, PARTS)), dma((2, 2, PARTS)), dma((2,)), dma((reach * CHUNKS,)), dma((2,)), dma((2,)), dma, dma,
    ]
    results = (
        ((rows, state), F32), ((rows, state), F32), ((heads, rows), F32), ((small, width), F32), ((1, small), F32)
    )
    kept = pl.pallas_call(
        functools.partial(kernel, nz, ny, nt),
        out_shape=tuple(vmem(*each) for each in results),
        in_specs=[pl.BlockSpec(memory_space=pl.ANY)] * 6,
        out_specs=(pl.BlockSpec(memory_space=pltpu.VMEM),) * 5,
        scratch_shapes=scratch,
        compiler_params=pltpu.CompilerParams(
            collective_id=0, has_side_effects=True, vmem_limit_bytes=56 * 1024 * 1024
        ),
    )(log_decay.T, out_grad, queries, key_rows, block_input, value_weight)
    query_grad, key_grad, decay_grad, weight_grad, norms = pl.pallas_call(
        put_out,
        out_shape=tuple(shape(*each) for each in results),
        in_specs=[pl.BlockSpec(memory_space=pltpu.VMEM)] * 5,
        out_specs=(pl.BlockSpec(memory_space=pl.ANY),) * 5,
        scratch_shapes=[dma((5,))],
    )(*(pltpu.with_memory_space_constraint(each, pltpu.VMEM) for each in kept))
    return query_grad, key_grad, decay_grad.T, weight_grad, norms.reshape(small)


def solution(mesh):
    nz = ny = 8
    nt = mesh.shape["tp"]
    split = Mesh(mesh.devices.reshape(nz, ny, nt), ("sp_0", "sp_1", "tp"))
    return jax.shard_map(
        functools.partial(on_device, nz, ny, nt),
        mesh=split,
        in_specs=(P(SP, None), P(None, "tp"), P(SP, "tp"), P(SP, "tp"), P(SP, "tp"), P(SP, "tp")),
        out_specs=(P(SP, "tp"), P(SP, "tp"), P(SP, "tp"), P(SP, "tp"), P(SP)),
        check_vma=False,
    )
```
